256 devices in a mesh: sp: 32 (over z, y), tp: 8 (over x, core).
Axes of the slice: x: 4, y: 4, z: 8, core: 2. Of those that a mesh axis runs over, the one named last changes fastest.
Arguments:
- tokens: bfloat16 [32768, 2048], P('sp'), may hold values from -6 to 6
- in_gain: float32 [2048], replicated, may hold values from 0.1 to 1.9
- w_query: bfloat16 [2048, 1024], P(None, 'tp'), may hold values from -0.125 to 0.125
- w_forget: bfloat16 [2048, 1024], P(None, 'tp'), may hold values from -0.125 to 0.125
- w_input: bfloat16 [2048, 1024], P(None, 'tp'), may hold values from -0.125 to 0.125
- w_outgate: bfloat16 [2048, 1024], P(None, 'tp'), may hold values from -0.125 to 0.125
- w_conv_h: bfloat16 [2048, 1024], P(None, 'tp'), may hold values from -0.125 to 0.125
- w_conv_b: bfloat16 [2048, 1024], P(None, 'tp'), may hold values from -0.125 to 0.125
- w_conv_c: bfloat16 [2048, 1024], P(None, 'tp'), may hold values from -0.125 to 0.125
- forget_floor: float32 [1024], P('tp'), may hold values from 0.84 to 1
- forget_leak: float32 [32768, 1024], P('sp', 'tp'), may hold values from -1 to 0
- state_gain: float32 [128], replicated, may hold values from 0.1 to 1.9
- conv_taps: bfloat16 [3, 1024], P(None, 'tp'), may hold values from -3.5 to 3.5
- group_gain: float32 [128], replicated, may hold values from 0.1 to 1.9
- out_state: bfloat16 [1024, 2048], P('tp'), may hold values from -0.1875 to 0.1875
- out_conv: bfloat16 [1024, 2048], P('tp'), may hold values from -0.1875 to 0.1875
Outputs:
- mixed_out: bfloat16 [32768, 2048], P('sp', 'tp')
The draws below stay inside these ranges and needn't reach their ends.
All inputs are finite; a program needn't handle non-finite values.
Results may differ from the reference program's by a relative error of at most 0.015.
Values may be sent and summed in bfloat16 or wider, within the bound.
A program may use at most 128 MiB of HBM per device.

```python
import jax
import jax.numpy as jnp
from jax import lax

D = 2048
GROUP_FEATURES = 128
MIXER_COUNT = 8
CONV_CH = 1024
BLOCK = 64
TAPS = 3
TOK_DEV = 1024
STEP_COUNT = 32768
STATE_W = 1024
MIX = 2048


def draw_forget_floor(key, part):
    key_fast, key_gap, key_slow = jax.random.split(jax.random.fold_in(key, 11), 3)
    share = 0.5
    is_fast = jax.random.uniform(key_fast, (MIXER_COUNT,)) < share
    is_fast = jnp.repeat(is_fast, GROUP_FEATURES)
    fast_gap = jnp.exp(jax.random.uniform(key_gap, (STATE_W,), jnp.float32, jnp.log(0.05), jnp.log(0.15)))
    slow_gap = jnp.exp(jax.random.uniform(key_slow, (STATE_W,), jnp.float32, jnp.log(0.2), jnp.log(1.0))) / STEP_COUNT
    return (1.0 - jnp.where(is_fast, fast_gap, slow_gap)).astype(jnp.float32)


def draw_forget_leak(key, part):
    key_scale, random_seed_site, key_depth, key_jitter = jax.random.split(jax.random.fold_in(key, 23), 4)
    nblk = STEP_COUNT // TOK_DEV
    low, high = (jnp.log(0.5), jnp.log(2.0))
    block_scale = jnp.exp(jax.random.uniform(key_scale, (nblk, MIXER_COUNT), jnp.float32, low, high))
    block_scale = jnp.repeat(jnp.repeat(block_scale, TOK_DEV, axis=0), GROUP_FEATURES, axis=1)
    jitter = jax.random.uniform(key_jitter, (STEP_COUNT, STATE_W), jnp.float32, 0.5, 1.5)
    starting_shift = -0.2 / STEP_COUNT * block_scale * jitter
    span_start = jax.random.randint(random_seed_site, (3, MIXER_COUNT), 0, STEP_COUNT)
    layer_number = jax.random.uniform(key_depth, (3, MIXER_COUNT), jnp.float32, jnp.log(0.5), jnp.log(0.8))
    element_places = jnp.arange(STEP_COUNT)[:, None]
    span_sizes = jnp.zeros((STEP_COUNT, MIXER_COUNT), jnp.float32)
    for entry_number in range(3):
        span_sizes = span_sizes + jnp.where(element_places == span_start[entry_number][None, :], layer_number[entry_number][None, :], 0.0)
    return (starting_shift + jnp.repeat(span_sizes, GROUP_FEATURES, axis=1)).astype(jnp.float32)


def with_spikes(values, key, source, target, parts, factor):
    owner, partner = [(jnp.arange(values.shape[position]) // (values.shape[position] // parts)).reshape([-1 if axis == position else 1 for axis in range(values.ndim)]) for position in (source, target)]
    chosen = jax.random.permutation(key, parts)[partner]
    strong = (owner == chosen) | (owner == (partner + parts // 2) % parts)
    return jnp.where(strong, factor * values, values)


def levels(key, dims, pieces, least, largest):
    level, own = 1.0, jax.random.fold_in(key, 6)
    for dim, parts in pieces:
        steps = jnp.exp(jax.random.uniform(jax.random.fold_in(own, dim), (parts,), jnp.float32, least / len(pieces), largest / len(pieces)))
        level = level * jnp.repeat(steps, dims[dim] // parts).reshape([-1 if axis == dim else 1 for axis in range(len(dims))])
    return level


def centred(rng, extent, spread, reach, cuts=(), held_as=jnp.bfloat16):
    loudness = levels(rng, extent, cuts, -0.22, 0.18) if cuts else 1.0
    array = jax.random.normal(rng, extent, jnp.float32) * spread * loudness
    return jnp.minimum(jnp.maximum(array, -reach), reach).astype(held_as)


def heavy_noise(own_key, dims, width, limit, shards, heavy, dtype=jnp.bfloat16):
    values = width * jax.random.normal(own_key, dims, jnp.float32)
    if shards:
        values = values * levels(own_key, dims, shards, -0.22, 0.18)
    return jnp.clip(with_spikes(values, jax.random.fold_in(own_key, 3), *heavy), -limit, limit).astype(dtype)


def setup_inputs(seed: int = 0) -> dict:
    streams_of = jax.random.split(jax.random.key(seed), 17)
    return {
        "tokens": centred(streams_of[0], (STEP_COUNT, D), 1.0, 6.0, ((0, 32),)),
        "in_gain": jnp.clip(1.0 + 0.18 * jax.random.normal(streams_of[1], (D,), jnp.float32), 0.1, 1.9),
        "w_query": centred(streams_of[2], (D, STATE_W), D ** -0.5, 0.125, ((1, 8),)),
        "w_forget": centred(streams_of[3], (D, STATE_W), D ** -0.5, 0.125, ((1, 8),)),
        "w_input": centred(streams_of[4], (D, STATE_W), D ** -0.5, 0.125, ((1, 8),)),
        "w_outgate": centred(streams_of[5], (D, STATE_W), D ** -0.5, 0.125, ((1, 8),)),
        "w_conv_h": centred(streams_of[6], (D, CONV_CH), D ** -0.5, 0.125, ((1, 8),)),
        "w_conv_b": centred(streams_of[7], (D, CONV_CH), D ** -0.5, 0.125, ((1, 8),)),
        "w_conv_c": centred(streams_of[8], (D, CONV_CH), D ** -0.5, 0.125, ((1, 8),)),
        "forget_floor": draw_forget_floor(jax.random.fold_in(streams_of[16], 71), 0),
        "forget_leak": draw_forget_leak(jax.random.fold_in(streams_of[16], 71), 0),
        "state_gain": jnp.clip(1.0 + 0.18 * jax.random.normal(streams_of[11], (GROUP_FEATURES,), jnp.float32), 0.1, 1.9),
        "conv_taps": centred(streams_of[12], (TAPS, CONV_CH), TAPS ** -0.5, 3.5, ((1, 8),)),
        "group_gain": jnp.clip(1.0 + 0.18 * jax.random.normal(streams_of[13], (GROUP_FEATURES,), jnp.float32), 0.1, 1.9),
        "out_state": heavy_noise(streams_of[14], (STATE_W, D), MIX ** -0.5, 0.1875, ((0, 8),), (0, 1, 8, 2.0)),
        "out_conv": heavy_noise(streams_of[15], (CONV_CH, D), MIX ** -0.5, 0.1875, ((0, 8),), (0, 1, 8, 2.0)),
    }


norm_eps = 1e-06
highest = lax.Precision.HIGHEST

def rms_rows(values, gain):
    scale = lax.rsqrt(lax.optimization_barrier(jnp.mean(values * values, axis=-1, keepdims=True)) + norm_eps)
    return values * scale * gain.astype(jnp.float32)

def state_block(carry_state, inputs):
    query_blk, key_blk, value_blk, logf_blk = inputs
    cum_log = jnp.cumsum(logf_blk, axis=1)
    carried = jnp.einsum('hcd,hde->hce', query_blk * jnp.exp(cum_log), carry_state, precision=highest)
    length = logf_blk.shape[1]
    causal = (jnp.arange(length)[:, None] >= jnp.arange(length)[None, :])[None, :, :, None]
    diff_log = cum_log[:, :, None, :] - cum_log[:, None, :, :]
    decay_all = jnp.exp(jnp.where(causal, diff_log, -jnp.inf))
    scores = jnp.einsum('hid,hjd,hijd->hij', query_blk, key_blk, decay_all, precision=highest)
    result = carried + jnp.einsum('hij,hje->hie', scores, value_blk, precision=highest)
    last_log = cum_log[:, -1, :]
    fresh = jnp.einsum('hcd,hce->hde', key_blk * jnp.exp(last_log[:, None, :] - cum_log), value_blk, precision=highest)
    new_state = jnp.exp(last_log)[:, :, None] * carry_state + fresh
    return (new_state, result)

def reference(tokens, in_gain, w_query, w_forget, w_input, w_outgate, w_conv_h, w_conv_b, w_conv_c, forget_floor, forget_leak, state_gain, conv_taps, group_gain, out_state, out_conv):
    count = tokens.shape[0]
    heads = MIXER_COUNT
    normed = rms_rows(tokens.astype(jnp.float32), in_gain).astype(jnp.bfloat16)

    def project(weight):
        return jnp.dot(normed, weight, preferred_element_type=jnp.float32).astype(jnp.bfloat16)
    proj_query = project(w_query)
    proj_forget = project(w_forget)
    proj_input = project(w_input)
    proj_outgate = project(w_outgate)
    proj_h = project(w_conv_h)
    proj_b = project(w_conv_b)
    proj_c = project(w_conv_c)
    gate_logit = proj_forget.astype(jnp.float32)
    log_forget = jnp.logaddexp(jnp.log(forget_floor), jnp.log1p(-forget_floor) + jax.nn.log_sigmoid(gate_logit)) + forget_leak
    key_gate = (1.0 - forget_floor) * jax.nn.sigmoid(-gate_logit)
    query_act = jax.nn.silu(proj_query.astype(jnp.float32))
    value_f = proj_input.astype(jnp.float32)
    nblk = count // BLOCK

    def to_blocks(arr):
        return arr.reshape(nblk, BLOCK, heads, GROUP_FEATURES).transpose(0, 2, 1, 3)
    start_state = jnp.zeros((heads, GROUP_FEATURES, GROUP_FEATURES), jnp.float32)
    _, outputs = lax.scan(state_block, start_state, (to_blocks(query_act), to_blocks(key_gate), to_blocks(value_f), to_blocks(log_forget)))
    state_read = outputs.transpose(0, 2, 1, 3).reshape(count, heads, GROUP_FEATURES)
    out_gate = jax.nn.silu(proj_outgate.astype(jnp.float32)).reshape(count, heads, GROUP_FEATURES)
    state_res = (rms_rows(state_read, state_gain) * out_gate).reshape(count, STATE_W).astype(jnp.bfloat16)
    conv_in = (proj_c.astype(jnp.float32) * proj_h.astype(jnp.float32)).astype(jnp.bfloat16)
    padded = jnp.concatenate([jnp.zeros((TAPS - 1, CONV_CH), jnp.bfloat16), conv_in], axis=0).astype(jnp.float32)
    taps_f = conv_taps.astype(jnp.float32)
    conv_sum = jnp.zeros((count, CONV_CH), jnp.float32)
    for offset in range(TAPS):
        conv_sum = conv_sum + taps_f[offset][None, :] * padded[offset:offset + count]
    gated = (proj_b.astype(jnp.float32) * conv_sum).reshape(count, CONV_CH // GROUP_FEATURES, GROUP_FEATURES)
    conv_res = rms_rows(gated, group_gain).reshape(count, CONV_CH).astype(jnp.bfloat16)
    total = jnp.dot(state_res, out_state, preferred_element_type=jnp.float32)
    total = total + jnp.dot(conv_res, out_conv, preferred_element_type=jnp.float32)
    return total.astype(jnp.bfloat16)
```

```python
import functools

import jax
import jax.numpy as jnp
from jax import lax
from jax.experimental import pallas as pl
from jax.experimental.pallas import tpu as pltpu
from jax.sharding import PartitionSpec as P

GROUP = 128
CHUNK = 128
ROWS = 256
TAPS = 3
HALO = 8
NY = 4
LOGS = 16

norm_eps = 1e-06
f32 = jnp.float32
bf16 = jnp.bfloat16


def dot(a, b, dims=((1,), (0,))):
    return lax.dot_general(a, b, (dims, ((), ())), preferred_element_type=f32)


def rms(values):
    return values * lax.rsqrt(jnp.mean(values * values, axis=-1, keepdims=True) + norm_eps)


def split3(values):
    hi = values.astype(bf16)
    rest = values - hi.astype(f32)
    mid = rest.astype(bf16)
    low = (rest - mid.astype(f32)).astype(bf16)
    return hi, mid, low


def fused_kernel(
    tp, ny, nz,
    tokens, in_gain, wq, wf, wi, wg, wh, wb, wc, floor, leak, state_gain, taps, group_gain,
    out_state, out_conv, result,
    tok, w, leakv, cols, mixed, kmid, val, emid, old, stats, gate, read, qdev,
    pad, state, offset, incoming, ybuf, zbuf, rim, tail, head_conv, head_gate,
    tok_sem, w_sem, leak_sem, own_sem,
    colx_send, colx_recv, coly_send, coly_recv,
    y_send, y_recv, z_send, z_recv, rim_send, rim_recv, blk_send, blk_recv,
):
    me, place = lax.axis_index("tp"), lax.axis_index("sp")
    sp = ny * nz
    core, chip = lax.rem(me, 2), lax.div(me, 2)
    partner = me + 1 - 2 * core
    yy, zz = lax.rem(place, ny), lax.div(place, ny)
    up, down, far = lax.rem(me + 2, tp), lax.rem(me + tp - 2, tp), lax.rem(me + 4, tp)
    ahead = lax.rem(me + tp + 2 - 4 * core, tp)
    behind = lax.rem(me + tp - 2 + 4 * core, tp)
    count, ncols = result.shape
    nb = count // ROWS
    nchunk = count // CHUNK
    part = GROUP // ny
    outs = (out_state, out_conv)

    def rows_at(t):
        return pl.ds(pl.multiple_of(t * ROWS, ROWS), ROWS)

    def tok_copy(t):
        return pltpu.make_async_copy(tokens.at[rows_at(t)], tok.at[rows_at(t)], tok_sem.at[t])

    weights = (wf, wi, wc, wh, wb, wg, wq)

    def w_copy(i):
        return pltpu.make_async_copy(weights[i], w.at[:, i * GROUP : (i + 1) * GROUP], w_sem.at[i])

    leak_copy = pltpu.make_async_copy(leak, leakv, leak_sem.at[0])

    def col_slice(target):
        return pl.ds(pl.multiple_of(target * ncols, ncols), ncols)

    mine_rows = pl.ds(pl.multiple_of(yy * part, part), part)

    def own_cols(kind):
        return pltpu.make_async_copy(
            outs[kind].at[:, col_slice(me)], cols.at[kind * tp + me], own_sem.at[kind]
        )

    def partner_cols(kind):
        return pltpu.make_async_remote_copy(
            outs[kind].at[:, col_slice(partner)], cols.at[kind * tp + me],
            colx_send.at[kind, 0], colx_recv.at[kind, me], device_id={"tp": partner},
        )

    def partner_cols_in(kind):
        return pltpu.make_async_remote_copy(
            outs[kind].at[:, col_slice(partner)], cols.at[kind * tp + partner],
            colx_send.at[kind, 0], colx_recv.at[kind, partner], device_id={"tp": partner},
        )

    def far_cols(kind, k):
        target = lax.rem(2 * chip + 2 + k, tp)
        return pltpu.make_async_remote_copy(
            outs[kind].at[mine_rows, col_slice(target)], cols.at[kind * tp + me, mine_rows],
            colx_send.at[kind, k + 1], colx_recv.at[kind, me], device_id={"tp": target},
        )

    def far_cols_in(kind, k):
        source = lax.rem(2 * chip + 2 + k, tp)
        return pltpu.make_async_remote_copy(
            outs[kind].at[mine_rows, col_slice(source)], cols.at[kind * tp + source, mine_rows],
            colx_send.at[kind, k + 1], colx_recv.at[kind, source], device_id={"tp": source},
        )

    def share_cols(kind, j, r):
        pair = pl.ds(kind * tp + lax.rem(2 * chip + 2 * j, tp), 2)
        ref = cols.at[pair, mine_rows]
        peer = lax.rem(yy + r, ny)
        return pltpu.make_async_remote_copy(
            ref, ref, coly_send.at[kind, j, r], coly_recv.at[kind, j, yy],
            device_id={"sp": zz * ny + peer},
        )

    def share_cols_in(kind, j, r):
        pair = pl.ds(kind * tp + lax.rem(2 * chip + 2 * j, tp), 2)
        peer = lax.rem(yy + r, ny)
        ref = cols.at[pair, pl.ds(pl.multiple_of(peer * part, part), part)]
        return pltpu.make_async_remote_copy(
            ref, ref, coly_send.at[kind, j, r], coly_recv.at[kind, j, peer],
            device_id={"sp": zz * ny + peer},
        )

    def y_copy(r):
        ref = ybuf.at[yy]
        return pltpu.make_async_remote_copy(
            ref, ref, y_send.at[r], y_recv.at[yy],
            device_id={"sp": zz * ny + lax.rem(yy + r, ny)},
        )

    def y_arrival(r):
        peer = lax.rem(yy + r, ny)
        ref = ybuf.at[peer]
        return pltpu.make_async_remote_copy(
            ref, ref, y_send.at[r], y_recv.at[peer], device_id={"sp": zz * ny + peer}
        )

    def z_copy(target):
        ref = zbuf.at[zz]
        return pltpu.make_async_remote_copy(
            ref, ref, z_send.at[target], z_recv.at[zz], device_id={"sp": target * ny + yy}
        )

    def z_arrival(source):
        ref = zbuf.at[source]
        return pltpu.make_async_remote_copy(
            ref, ref, z_send.at[source], z_recv.at[source], device_id={"sp": source * ny + yy}
        )

    rim_copy = pltpu.make_async_remote_copy(
        tail, rim, rim_send.at[0], rim_recv.at[0], device_id={"sp": lax.rem(place + 1, sp)}
    )

    def block_copy(kind, t, origin, target, slot):
        lanes = pl.ds(pl.multiple_of((kind * tp + origin) * GROUP, GROUP), GROUP)
        ref = mixed.at[t, :, lanes]
        return pltpu.make_async_remote_copy(
            ref, ref, blk_send.at[kind, slot, t], blk_recv.at[kind, origin, t],
            device_id={"tp": target},
        )

    def own_copies(kind, t):
        return [
            block_copy(kind, t, me, ahead, 1),
            block_copy(kind, t, me, behind, 2),
            block_copy(kind, t, me, partner, 0),
        ]

    def near_relays(kind, t):
        return [
            block_copy(kind, t, behind, ahead, 3),
            block_copy(kind, t, behind, partner, 4),
            block_copy(kind, t, ahead, partner, 5),
        ]

    def far_relay(kind, t):
        return block_copy(kind, t, far, partner, 6)

    def arrival(kind, t, origin):
        return block_copy(kind, t, origin, partner, 0)

    def relay_first(kind, t):
        first, second, third = near_relays(kind, t)
        arrival(kind, t, behind).wait_recv()
        first.start()
        second.start()
        arrival(kind, t, ahead).wait_recv()
        third.start()

    def relay_second(kind, t):
        arrival(kind, t, far).wait_recv()
        far_relay(kind, t).start()

    def put(kind, t, value):
        lanes = pl.ds(pl.multiple_of((kind * tp + me) * GROUP, GROUP), GROUP)
        mixed[t, :, lanes] = value

    for i in (0, 1):
        w_copy(i).start()
    tok_copy(0).start()
    leak_copy.start()
    for t in range(1, nb):
        tok_copy(t).start()
    for i in range(2, 7):
        w_copy(i).start()
    barrier = pltpu.get_barrier_semaphore()
    for k in range(1, tp):
        pl.semaphore_signal(barrier, inc=1, device_id={"tp": lax.rem(me + k, tp)})
    for r in range(1, ny):
        pl.semaphore_signal(barrier, inc=1, device_id={"sp": zz * ny + lax.rem(yy + r, ny)})
    for r in range(1, nz):
        pl.semaphore_signal(barrier, inc=1, device_id={"sp": lax.rem(zz + r, nz) * ny + yy})
    pl.semaphore_signal(barrier, inc=1, device_id={"sp": lax.rem(place + 1, sp)})
    pl.semaphore_signal(barrier, inc=1, device_id={"sp": lax.rem(place + sp - 1, sp)})
    pl.semaphore_wait(barrier, tp + ny + nz - 3 + 2)
    for kind in range(2):
        for k in range(tp - 2):
            far_cols(kind, k).start()
    for kind in range(2):
        partner_cols(kind).start()
        own_cols(kind).start()
    pad[0:HALO, :] = jnp.zeros((HALO, GROUP), f32)
    state[...] = jnp.zeros_like(state)
    offset[...] = jnp.zeros_like(offset)

    row = lax.broadcasted_iota(jnp.int32, (CHUNK, CHUNK), 0)
    col = lax.broadcasted_iota(jnp.int32, (CHUNK, CHUNK), 1)
    causal = row >= col
    ones = causal.astype(bf16)

    w_copy(0).wait()
    w_copy(1).wait()
    leak_copy.wait()

    def states(t, _):
        here = rows_at(t)
        tok_copy(t).wait()
        normed = (rms(tok[here, :].astype(f32)) * in_gain[...]).astype(bf16)
        tok[here, :] = normed
        both = dot(normed, w[:, 0 : 2 * GROUP])
        x = both[:, :GROUP].astype(bf16).astype(f32)
        value = both[:, GROUP:].astype(bf16)
        val[here, :] = value
        key = (1.0 - floor[...]) * jax.nn.sigmoid(-x)
        logf = jnp.log(1.0 - key) + leakv[here, :]
        for b in range(ROWS // CHUNK):
            lo, hi = b * CHUNK, (b + 1) * CHUNK
            at = pl.ds(pl.multiple_of(t * ROWS + lo, CHUNK), CHUNK)
            chunk = t * (ROWS // CHUNK) + b
            sums = dot(ones, jnp.concatenate(split3(logf[lo:hi]), axis=1))
            cum = sums[:, :GROUP] + sums[:, GROUP : 2 * GROUP] + sums[:, 2 * GROUP :]
            mid = cum[CHUNK // 2 - 1 : CHUNK // 2]
            last = cum[CHUNK - 1 : CHUNK]
            emid[at, :] = jnp.exp(cum - mid)
            k_mid = key[lo:hi] * jnp.exp(mid - cum)
            kmid[at, :] = k_mid.astype(bf16)
            k_end = (k_mid * jnp.exp(last - mid)).astype(bf16)
            held = state[...]
            old[chunk] = held.astype(bf16)
            stats[chunk, 0:1] = mid
            stats[chunk, 1:2] = offset[0:1, :]
            state[...] = held * jnp.exp(last) + dot(value[lo:hi], k_end, ((0,), (0,)))
            offset[...] += last
        return 0

    lax.fori_loop(0, nb, states, 0)

    def pack(slot, matrix, logs):
        hi, mid, low = split3(logs)
        slot[0:GROUP, :] = matrix.astype(bf16)
        r = lax.broadcasted_iota(jnp.int32, (LOGS, GROUP), 0)
        rows = jnp.where(r == 0, hi.astype(f32), jnp.where(r == 1, mid.astype(f32), low.astype(f32)))
        slot[GROUP : GROUP + LOGS, :] = rows.astype(bf16)

    def unpack(slot):
        logs = slot[GROUP : GROUP + LOGS, :].astype(f32)
        return slot[0:GROUP, :].astype(f32), logs[0:1] + logs[1:2] + logs[2:3]

    pack(ybuf.at[yy], state[...], offset[0:1, :])
    for r in range(1, ny):
        y_copy(r).start()

    for i in range(2, 6):
        w_copy(i).wait()
    taps_f = taps[...].astype(f32)

    def conv_block(t, _):
        here = rows_at(t)
        normed = tok[here, :]
        first = dot(normed, w[:, 2 * GROUP : 4 * GROUP])
        second = dot(normed, w[:, 4 * GROUP : 6 * GROUP])
        conv_in = first[:, :GROUP].astype(bf16).astype(f32) * first[:, GROUP:].astype(bf16).astype(f32)
        conv_in = conv_in.astype(bf16).astype(f32)
        proj_b = second[:, :GROUP].astype(bf16).astype(f32)
        gate[here, :] = second[:, GROUP:].astype(bf16)
        pad[HALO : HALO + ROWS, :] = conv_in
        total = taps_f[TAPS - 1 : TAPS] * conv_in
        for j in range(TAPS - 1):
            total += taps_f[j : j + 1] * pad[HALO - (TAPS - 1) + j : HALO - (TAPS - 1) + j + ROWS, :]
        put(1, t, (rms(proj_b * total) * group_gain[...]).astype(bf16))

        @pl.when(t == 0)
        def _():
            head_conv[...] = conv_in[:HALO]
            head_gate[...] = proj_b[:HALO]

        pad[0:HALO, :] = conv_in[ROWS - HALO :]

        @pl.when(t > 0)
        def _():
            for copy in own_copies(1, t):
                copy.start()

        return 0

    half = nb // 2
    lax.fori_loop(0, half, conv_block, 0)

    for r in range(1, ny):
        y_arrival(r).wait_recv()
    whole, logs = unpack(ybuf.at[0])
    for j in range(1, ny):
        more, log = unpack(ybuf.at[j])
        whole = whole * jnp.exp(log) + more
        logs = logs + log
    pack(zbuf.at[zz], whole, logs)

    def send_z(target, _):
        z_copy(target).start()
        return 0

    lax.fori_loop(zz + 1, nz, send_z, 0)

    lax.fori_loop(half, nb, conv_block, 0)
    tail[...] = pad[0:HALO, :]
    rim_copy.start()

    for kind in range(2):
        for k in range(tp - 2):
            far_cols_in(kind, k).wait_recv()
    for r in range(1, ny):
        for kind in range(2):
            for j in range(1, tp // 2):
                share_cols(kind, j, r).start()

    w_copy(6).wait()

    def reads(t, _):
        here = rows_at(t)

        @pl.when(t > 0)
        def _():
            relay_first(1, t)

        query = jax.nn.silu(dot(tok[here, :], w[:, 6 * GROUP : 7 * GROUP]).astype(bf16).astype(f32))
        for b in range(ROWS // CHUNK):
            lo, hi = b * CHUNK, (b + 1) * CHUNK
            at = pl.ds(pl.multiple_of(t * ROWS + lo, CHUNK), CHUNK)
            chunk = t * (ROWS // CHUNK) + b
            mid, before = stats[chunk, 0:1], stats[chunk, 1:2]
            q_mid = query[lo:hi] * emid[at, :]
            q_all = q_mid * jnp.exp(mid)
            qdev[at, :] = (q_all * jnp.exp(before)).astype(bf16)
            scores = dot(q_mid.astype(bf16), kmid[at, :], ((1,), (1,)))
            scores = jnp.where(causal, scores, 0.0).astype(bf16)
            read[at, :] = dot(scores, val[at, :]) + dot(q_all.astype(bf16), old[chunk], ((1,), (1,)))
        return 0

    lax.fori_loop(0, nb, reads, 0)

    rim_copy.wait_recv()
    before = jnp.where(place > 0, rim[...], 0.0)
    ext = jnp.concatenate([before, head_conv[...]], axis=0)
    fixed = taps_f[TAPS - 1 : TAPS] * head_conv[...]
    for j in range(TAPS - 1):
        fixed += taps_f[j : j + 1] * ext[HALO - (TAPS - 1) + j : 2 * HALO - (TAPS - 1) + j]
    fixed = rms(head_gate[...] * fixed) * group_gain[...]
    mixed[0, 0:HALO, pl.ds(pl.multiple_of((tp + me) * GROUP, GROUP), GROUP)] = fixed.astype(bf16)
    for copy in own_copies(1, 0):
        copy.start()

    incoming[...] = jnp.zeros_like(incoming)

    def hop_z(source, _):
        z_arrival(source).wait_recv()
        matrix, log = unpack(zbuf.at[source])
        incoming[...] = incoming[...] * jnp.exp(log) + matrix
        return 0

    lax.fori_loop(0, zz, hop_z, 0)

    def hop_y(source, _):
        matrix, log = unpack(ybuf.at[source])
        incoming[...] = incoming[...] * jnp.exp(log) + matrix
        return 0

    lax.fori_loop(0, yy, hop_y, 0)

    def merge(t, _):
        here = rows_at(t)
        total = read[here, :] + dot(qdev[here, :], incoming[...].astype(bf16), ((1,), (1,)))
        out = rms(total) * state_gain[...] * jax.nn.silu(gate[here, :].astype(f32))
        put(0, t, out.astype(bf16))
        for copy in own_copies(0, t):
            copy.start()
        return 0

    lax.fori_loop(0, nb, merge, 0)

    relay_first(1, 0)

    def relay_conv(t, _):
        relay_second(1, t + 1)
        return 0

    lax.fori_loop(0, nb - 1, relay_conv, 0)

    def relay_state(t, _):
        relay_first(0, t)
        return 0

    lax.fori_loop(0, nb, relay_state, 0)
    relay_second(1, 0)

    for kind in range(2):
        own_cols(kind).wait()
        partner_cols_in(kind).wait_recv()
        for r in range(1, ny):
            for j in range(1, tp // 2):
                share_cols_in(kind, j, r).wait_recv()

    def finish(t, _):
        relay_second(0, t)
        for kind in range(2):
            for k in range(tp // 2):
                arrival(kind, t, lax.rem(partner + 2 * k, tp)).wait_recv()
        result[rows_at(t), :] = dot(mixed[t], cols[...].reshape(2 * tp * GROUP, ncols)).astype(bf16)
        return 0

    lax.fori_loop(0, nb, finish, 0)

    def drain(t, _):
        for kind in range(2):
            for copy in own_copies(kind, t) + near_relays(kind, t) + [far_relay(kind, t)]:
                copy.wait_send()
        return 0

    lax.fori_loop(0, nb, drain, 0)
    for kind in range(2):
        partner_cols(kind).wait_send()
        for k in range(tp - 2):
            far_cols(kind, k).wait_send()
        for r in range(1, ny):
            for j in range(1, tp // 2):
                share_cols(kind, j, r).wait_send()
    for r in range(1, ny):
        y_copy(r).wait_send()

    def drain_z(target, _):
        z_copy(target).wait_send()
        return 0

    lax.fori_loop(zz + 1, nz, drain_z, 0)
    rim_copy.wait_send()


def body(
    tokens, in_gain, w_query, w_forget, w_input, w_outgate, w_conv_h, w_conv_b, w_conv_c,
    forget_floor, forget_leak, state_gain, conv_taps, group_gain, out_state, out_conv,
):
    count, feats = tokens.shape
    tp, sp = lax.axis_size("tp"), lax.axis_size("sp")
    ny, nz = NY, sp // NY
    ncols, nb = out_state.shape[1] // tp, count // ROWS
    nchunk = count // CHUNK
    hbm, vmem = pl.BlockSpec(memory_space=pl.ANY), pl.BlockSpec(memory_space=pltpu.VMEM)
    sems = pltpu.SemaphoreType.DMA
    return pl.pallas_call(
        functools.partial(fused_kernel, tp, ny, nz),
        in_specs=[hbm, vmem] + [hbm] * 7 + [vmem, hbm, vmem, vmem, vmem, hbm, hbm],
        out_specs=vmem,
        out_shape=jax.ShapeDtypeStruct((count, ncols), bf16),
        scratch_shapes=[
            pltpu.VMEM((count, feats), bf16),
            pltpu.VMEM((feats, 7 * GROUP), bf16),
            pltpu.VMEM((count, GROUP), f32),
            pltpu.VMEM((2 * tp, GROUP, ncols), bf16),
            pltpu.VMEM((nb, ROWS, 2 * tp * GROUP), bf16),
            pltpu.VMEM((count, GROUP), bf16),
            pltpu.VMEM((count, GROUP), bf16),
            pltpu.VMEM((count, GROUP), f32),
            pltpu.VMEM((nchunk, GROUP, GROUP), bf16),
            pltpu.VMEM((nchunk, HALO, GROUP), f32),
            pltpu.VMEM((count, GROUP), bf16),
            pltpu.VMEM((count, GROUP), f32),
            pltpu.VMEM((count, GROUP), bf16),
            pltpu.VMEM((HALO + ROWS, GROUP), f32),
            pltpu.VMEM((GROUP, GROUP), f32),
            pltpu.VMEM((HALO, GROUP), f32),
            pltpu.VMEM((GROUP, GROUP), f32),
            pltpu.VMEM((ny, GROUP + LOGS, GROUP), bf16),
            pltpu.VMEM((nz, GROUP + LOGS, GROUP), bf16),
            pltpu.VMEM((HALO, GROUP), f32),
            pltpu.VMEM((HALO, GROUP), f32),
            pltpu.VMEM((HALO, GROUP), f32),
            pltpu.VMEM((HALO, GROUP), f32),
            sems((nb,)), sems((7,)), sems((1,)), sems((2,)),
            sems((2, tp)), sems((2, tp)), sems((2, tp // 2, ny)), sems((2, tp // 2, ny)),
            sems((ny,)), sems((ny,)), sems((nz,)), sems((nz,)), sems((1,)), sems((1,)),
            sems((2, 7, nb)), sems((2, tp, nb)),
        ],
        compiler_params=pltpu.CompilerParams(
            vmem_limit_bytes=48 * 2**20, collective_id=0, has_side_effects=True
        ),
    )(
        tokens, in_gain[None], w_query, w_forget, w_input, w_outgate, w_conv_h, w_conv_b, w_conv_c,
        forget_floor[None], forget_leak, state_gain[None], conv_taps, group_gain[None],
        out_state, out_conv,
    )


def solution(mesh):
    cols, rows = P(None, "tp"), P("tp", None)
    in_specs = (
        P("sp", None), P(), cols, cols, cols, cols, cols, cols, cols,
        P("tp"), P("sp", "tp"), P(), cols, P(), rows, rows,
    )
    return jax.shard_map(
        body, mesh=mesh, in_specs=in_specs, out_specs=P("sp", "tp"), check_vma=False
    )
```

```python
import functools

import jax
import jax.numpy as jnp
from jax import lax
from jax.experimental import pallas as pl
from jax.experimental.pallas import tpu as pltpu
from jax.sharding import PartitionSpec as P

GROUP = 128
CHUNK = 128
ROWS = 256
TAPS = 3
HALO = 8
NY = 4
LOGS = 16

norm_eps = 1e-06
f32 = jnp.float32
bf16 = jnp.bfloat16


scope = jax.named_scope


def dot(a, b, dims=((1,), (0,))):
    return lax.dot_general(a, b, (dims, ((), ())), preferred_element_type=f32)


def rms(values):
    return values * lax.rsqrt(jnp.mean(values * values, axis=-1, keepdims=True) + norm_eps)


def split3(values):
    hi = values.astype(bf16)
    rest = values - hi.astype(f32)
    mid = rest.astype(bf16)
    low = (rest - mid.astype(f32)).astype(bf16)
    return hi, mid, low


def fused_kernel(
    tp, ny, nz,
    tokens, in_gain, wq, wf, wi, wg, wh, wb, wc, floor, leak, state_gain, taps, group_gain,
    out_state, out_conv, result,
    tok, w, leakv, cols, mixed, kmid, val, emid, old, stats, gate, read, qdev, scl, outv,
    gainv, floorv, sgainv, ggainv, tapsv,
    pad, incoming, ybuf, zbuf, rim, tail, head_gate,
    tok_sem, w_sem, small_sem, own_sem, out_sem, ready_z, ready_rim,
    colx_send, colx_recv, coly_send, coly_recv,
    y_send, y_recv, z_send, z_recv, rim_send, rim_recv, blk_send, blk_recv,
):
    me, place = lax.axis_index("tp"), lax.axis_index("sp")
    sp = ny * nz
    core, chip = lax.rem(me, 2), lax.div(me, 2)
    partner = me + 1 - 2 * core
    yy, zz = lax.rem(place, ny), lax.div(place, ny)
    far = lax.rem(me + 4, tp)
    ahead = lax.rem(me + tp + 2 - 4 * core, tp)
    behind = lax.rem(me + tp - 2 + 4 * core, tp)
    count, ncols = result.shape
    nb = count // ROWS
    nchunk = count // CHUNK
    part = GROUP // ny
    per = ROWS // CHUNK
    outs = (out_state, out_conv)

    def rows_at(t):
        return pl.ds(pl.multiple_of(t * ROWS, ROWS), ROWS)

    def tok_copy(t):
        return pltpu.make_async_copy(tokens.at[rows_at(t)], tok.at[rows_at(t)], tok_sem.at[t])

    weights = (wf, wi, wc, wh, wb, wg, wq)

    def w_copy(i):
        return pltpu.make_async_copy(weights[i], w.at[:, i * GROUP : (i + 1) * GROUP], w_sem.at[i])

    smalls = (
        pltpu.make_async_copy(in_gain, gainv, small_sem.at[0]),
        pltpu.make_async_copy(floor, floorv, small_sem.at[1]),
        pltpu.make_async_copy(leak, leakv, small_sem.at[2]),
        pltpu.make_async_copy(taps, tapsv, small_sem.at[3]),
        pltpu.make_async_copy(group_gain, ggainv, small_sem.at[4]),
        pltpu.make_async_copy(state_gain, sgainv, small_sem.at[5]),
    )

    def out_copy(t):
        return pltpu.make_async_copy(outv.at[rows_at(t)], result.at[rows_at(t)], out_sem.at[t])

    def col_slice(target):
        return pl.ds(pl.multiple_of(target * ncols, ncols), ncols)

    mine_rows = pl.ds(pl.multiple_of(yy * part, part), part)

    def own_cols(kind):
        return pltpu.make_async_copy(
            outs[kind].at[:, col_slice(me)], cols.at[kind * tp + me], own_sem.at[kind]
        )

    def partner_cols(kind):
        return pltpu.make_async_remote_copy(
            outs[kind].at[:, col_slice(partner)], cols.at[kind * tp + me],
            colx_send.at[kind, 0], colx_recv.at[kind, me], device_id={"tp": partner},
        )

    def partner_cols_in(kind):
        return pltpu.make_async_remote_copy(
            outs[kind].at[:, col_slice(partner)], cols.at[kind * tp + partner],
            colx_send.at[kind, 0], colx_recv.at[kind, partner], device_id={"tp": partner},
        )

    def far_cols(kind, k):
        target = lax.rem(2 * chip + 2 + k, tp)
        return pltpu.make_async_remote_copy(
            outs[kind].at[mine_rows, col_slice(target)], cols.at[kind * tp + me, mine_rows],
            colx_send.at[kind, k + 1], colx_recv.at[kind, me], device_id={"tp": target},
        )

    def far_cols_in(kind, k):
        source = lax.rem(2 * chip + 2 + k, tp)
        return pltpu.make_async_remote_copy(
            outs[kind].at[mine_rows, col_slice(source)], cols.at[kind * tp + source, mine_rows],
            colx_send.at[kind, k + 1], colx_recv.at[kind, source], device_id={"tp": source},
        )

    def share_cols(kind, j, r):
        pair = pl.ds(kind * tp + lax.rem(2 * chip + 2 * j, tp), 2)
        ref = cols.at[pair, mine_rows]
        peer = lax.rem(yy + r, ny)
        return pltpu.make_async_remote_copy(
            ref, ref, coly_send.at[kind, j, r], coly_recv.at[kind, j, yy],
            device_id={"sp": zz * ny + peer},
        )

    def share_cols_in(kind, j, r):
        pair = pl.ds(kind * tp + lax.rem(2 * chip + 2 * j, tp), 2)
        peer = lax.rem(yy + r, ny)
        ref = cols.at[pair, pl.ds(pl.multiple_of(peer * part, part), part)]
        return pltpu.make_async_remote_copy(
            ref, ref, coly_send.at[kind, j, r], coly_recv.at[kind, j, peer],
            device_id={"sp": zz * ny + peer},
        )

    def y_copy(r):
        ref = ybuf.at[yy]
        return pltpu.make_async_remote_copy(
            ref, ref, y_send.at[r], y_recv.at[yy],
            device_id={"sp": zz * ny + lax.rem(yy + r, ny)},
        )

    def y_arrival(r):
        peer = lax.rem(yy + r, ny)
        ref = ybuf.at[peer]
        return pltpu.make_async_remote_copy(
            ref, ref, y_send.at[r], y_recv.at[peer], device_id={"sp": zz * ny + peer}
        )

    def z_copy(target):
        ref = zbuf.at[zz]
        return pltpu.make_async_remote_copy(
            ref, ref, z_send.at[target], z_recv.at[zz], device_id={"sp": target * ny + yy}
        )

    def z_arrival(source):
        ref = zbuf.at[source]
        return pltpu.make_async_remote_copy(
            ref, ref, z_send.at[source], z_recv.at[source], device_id={"sp": source * ny + yy}
        )

    rim_copy = pltpu.make_async_remote_copy(
        tail, rim, rim_send.at[0], rim_recv.at[0], device_id={"sp": place + 1}
    )
    rim_arrival = pltpu.make_async_remote_copy(
        tail, rim, rim_send.at[0], rim_recv.at[0], device_id={"sp": place - 1}
    )

    def block_copy(kind, t, origin, target, slot):
        lanes = pl.ds(pl.multiple_of((kind * tp + origin) * GROUP, GROUP), GROUP)
        ref = mixed.at[t, :, lanes]
        return pltpu.make_async_remote_copy(
            ref, ref, blk_send.at[kind, slot, t], blk_recv.at[kind, origin, t],
            device_id={"tp": target},
        )

    def own_copies(kind, t):
        return [
            block_copy(kind, t, me, ahead, 1),
            block_copy(kind, t, me, behind, 2),
            block_copy(kind, t, me, partner, 0),
        ]

    def near_relays(kind, t):
        return [
            block_copy(kind, t, behind, ahead, 3),
            block_copy(kind, t, behind, partner, 4),
            block_copy(kind, t, ahead, partner, 5),
        ]

    def far_relay(kind, t):
        return block_copy(kind, t, far, partner, 6)

    def arrival(kind, t, origin):
        return block_copy(kind, t, origin, partner, 0)

    def relay_first(kind, t):
        first, second, third = near_relays(kind, t)
        arrival(kind, t, behind).wait_recv()
        first.start()
        second.start()
        arrival(kind, t, ahead).wait_recv()
        third.start()

    def relay_second(kind, t):
        arrival(kind, t, far).wait_recv()
        far_relay(kind, t).start()

    def put(kind, t, value):
        lanes = pl.ds(pl.multiple_of((kind * tp + me) * GROUP, GROUP), GROUP)
        mixed[t, :, lanes] = value

    smalls[0].start()
    tok_copy(0).start()
    w_copy(0).start()
    w_copy(1).start()
    smalls[1].start()
    smalls[2].start()
    for t in range(1, nb):
        tok_copy(t).start()
    barrier = pltpu.get_barrier_semaphore()
    for k in range(1, tp):
        pl.semaphore_signal(barrier, inc=1, device_id={"tp": lax.rem(me + k, tp)})
    for r in range(1, ny):
        pl.semaphore_signal(barrier, inc=1, device_id={"sp": zz * ny + lax.rem(yy + r, ny)})

    def greet_z(target, _):
        pl.semaphore_signal(barrier, inc=1, device_id={"sp": target * ny + yy})
        return 0

    lax.fori_loop(zz + 1, nz, greet_z, 0)

    @pl.when(place < sp - 1)
    def _():
        pl.semaphore_signal(barrier, inc=1, device_id={"sp": place + 1})

    for i in range(2, 7):
        w_copy(i).start()
    for copy in smalls[3:]:
        copy.start()
    with scope("barrier"):
        pl.semaphore_wait(barrier, tp + ny - 2 + zz + jnp.minimum(place, 1))

    def ready(target, _):
        pl.semaphore_signal(ready_z.at[0], inc=1, device_id={"sp": target * ny + yy})
        return 0

    lax.fori_loop(0, zz, ready, 0)

    @pl.when(place > 0)
    def _():
        pl.semaphore_signal(ready_rim.at[0], inc=1, device_id={"sp": place - 1})

    for kind in range(2):
        for k in range(tp - 2):
            far_cols(kind, k).start()
    for kind in range(2):
        partner_cols(kind).start()
        own_cols(kind).start()

    row = lax.broadcasted_iota(jnp.int32, (CHUNK, CHUNK), 0)
    col = lax.broadcasted_iota(jnp.int32, (CHUNK, CHUNK), 1)
    causal = row >= col
    ones = causal.astype(bf16)

    def lanes(first, last):
        return slice(first * GROUP, last * GROUP)

    def project_states(t):
        here = slice(t * ROWS, (t + 1) * ROWS)
        with scope("tokwait"):
            tok_copy(t).wait()
        raw = tok[here, :]
        scaled = raw * gainv[...].astype(bf16)
        tok[here, :] = scaled
        squares = raw * raw
        width = squares.shape[1] // 2
        squares = (squares[:, :width] + squares[:, width:]).astype(f32)
        mean = jnp.sum(squares, axis=1, keepdims=True) * (1.0 / raw.shape[1])
        scale = jnp.broadcast_to(lax.rsqrt(mean + norm_eps), (ROWS, GROUP))
        scl[here, :] = scale
        both = dot(scaled, w[:, lanes(0, 2)])
        x = (both[:, :GROUP] * scale).astype(bf16)
        value = (both[:, GROUP:] * scale).astype(bf16)
        return x, value

    def chain(t, x, value, carry):
        state, offset = carry
        val[slice(t * ROWS, (t + 1) * ROWS), :] = value
        key = (1.0 - floorv[...]) * jax.nn.sigmoid(-x.astype(f32))
        logf = jnp.log(1.0 - key) + leakv[slice(t * ROWS, (t + 1) * ROWS), :]
        for b in range(per):
            lo, hi = b * CHUNK, (b + 1) * CHUNK
            at = slice(t * ROWS + lo, t * ROWS + hi)
            chunk = t * per + b
            sums = dot(ones, jnp.concatenate(split3(logf[lo:hi]), axis=1))
            cum = sums[:, :GROUP] + sums[:, GROUP : 2 * GROUP] + sums[:, 2 * GROUP :]
            mid = cum[CHUNK // 2 - 1 : CHUNK // 2]
            last = cum[CHUNK - 1 : CHUNK]
            emid[at, :] = jnp.exp(cum - mid)
            k_mid = key[lo:hi] * jnp.exp(mid - cum)
            kmid[at, :] = k_mid.astype(bf16)
            k_end = (k_mid * jnp.exp(last - mid)).astype(bf16)
            old[chunk] = state.astype(bf16)
            stats[chunk, 0:1] = mid
            stats[chunk, 1:2] = offset
            state = state * jnp.exp(last) + dot(value[lo:hi], k_end, ((0,), (0,)))
            offset = offset + last
        return state, offset

    carry = (jnp.zeros((GROUP, GROUP), f32), jnp.zeros((1, GROUP), f32))
    with scope("w01wait"):
        smalls[0].wait()
        w_copy(0).wait()
        w_copy(1).wait()
    with scope("A"):
        held = project_states(0)
        smalls[1].wait()
        smalls[2].wait()
        for t in range(1, nb):
            more = project_states(t)
            carry = chain(t - 1, *held, carry)
            held = more
        carry = chain(nb - 1, *held, carry)

    def pack(slot, matrix, logs):
        hi, mid, low = split3(logs)
        slot[0:GROUP, :] = matrix.astype(bf16)
        r = lax.broadcasted_iota(jnp.int32, (LOGS, GROUP), 0)
        rows = jnp.where(r == 0, hi.astype(f32), jnp.where(r == 1, mid.astype(f32), low.astype(f32)))
        slot[GROUP : GROUP + LOGS, :] = rows.astype(bf16)

    def unpack(slot):
        logs = slot[GROUP : GROUP + LOGS, :].astype(f32)
        return slot[0:GROUP, :].astype(f32), logs[0:1] + logs[1:2] + logs[2:3]

    pack(ybuf.at[yy], *carry)
    for r in range(1, ny):
        y_copy(r).start()

    with scope("w23wait"):
        w_copy(2).wait()
        w_copy(3).wait()

    def gated_inputs(here):
        both = dot(tok[here, :], w[:, lanes(2, 4)])
        factor = scl[here, :]
        left = (both[:, :GROUP] * factor).astype(bf16).astype(f32)
        right = (both[:, GROUP:] * factor).astype(bf16).astype(f32)
        return (left * right).astype(bf16).astype(f32)

    with scope("rimsend"):
        tail[...] = gated_inputs(slice(count - 2 * HALO, count))[HALO:]

        @pl.when(place < sp - 1)
        def _():
            pl.semaphore_wait(ready_rim.at[0], 1)
            rim_copy.start()

    with scope("w45wait"):
        w_copy(4).wait()
        w_copy(5).wait()
        for copy in smalls[3:]:
            copy.wait()
    taps_f = tapsv[...].astype(f32)
    pad[0:HALO, :] = jnp.zeros((HALO, GROUP), f32)

    def convolve(first, size, conv_in, proj_b):
        total = taps_f[TAPS - 1 : TAPS] * conv_in
        for j in range(TAPS - 1):
            start = HALO - (TAPS - 1) + j + first
            total += taps_f[j : j + 1] * pad[start : start + size, :]
        return (rms(proj_b * total) * ggainv[...]).astype(bf16)

    def conv_block(t):
        here = slice(t * ROWS, (t + 1) * ROWS)
        conv_in = gated_inputs(here)
        pad[HALO + t * ROWS : HALO + (t + 1) * ROWS, :] = conv_in
        both = dot(tok[here, :], w[:, lanes(4, 6)])
        factor = scl[here, :]
        proj_b = (both[:, :GROUP] * factor).astype(bf16).astype(f32)
        gate[here, :] = (both[:, GROUP:] * factor).astype(bf16)
        if t == 0:
            head_gate[...] = proj_b[: 2 * HALO]
        put(1, t, convolve(t * ROWS, ROWS, conv_in, proj_b))

    def send(kind, t):
        for copy in own_copies(kind, t):
            copy.start()

    with scope("B01"):
        conv_block(0)
        conv_block(1)
        send(1, 1)

    with scope("rimwait"):
        @pl.when(place > 0)
        def _():
            rim_arrival.wait_recv()
            pad[0:HALO, :] = rim[...]

    fixed = convolve(0, 2 * HALO, pad[HALO : 3 * HALO, :], head_gate[...])
    mixed[0, 0 : 2 * HALO, pl.ds(pl.multiple_of((tp + me) * GROUP, GROUP), GROUP)] = fixed
    send(1, 0)

    with scope("ywait"):
        for r in range(1, ny):
            y_arrival(r).wait_recv()
    whole, logs = unpack(ybuf.at[0])
    for j in range(1, ny):
        more, log = unpack(ybuf.at[j])
        whole = whole * jnp.exp(log) + more
        logs = logs + log
    pack(zbuf.at[zz], whole, logs)
    with scope("readyz"):
        @pl.when(zz < nz - 1)
        def _():
            pl.semaphore_wait(ready_z.at[0], nz - 1 - zz)

    def send_z(target, _):
        z_copy(target).start()
        return 0

    lax.fori_loop(zz + 1, nz, send_z, 0)

    with scope("B23"):
        for t in range(2, nb):
            conv_block(t)
            send(1, t)

    with scope("colxwait"):
        for kind in range(2):
            for k in range(tp - 2):
                far_cols_in(kind, k).wait_recv()
    for r in range(1, ny):
        for kind in range(2):
            for j in range(1, tp // 2):
                share_cols(kind, j, r).start()

    with scope("w6wait"):
        w_copy(6).wait()

    def reads(t):
        here = slice(t * ROWS, (t + 1) * ROWS)
        x = (dot(tok[here, :], w[:, lanes(6, 7)]) * scl[here, :]).astype(bf16).astype(f32)
        query = jax.nn.silu(x)
        for b in range(per):
            lo, hi = b * CHUNK, (b + 1) * CHUNK
            at = slice(t * ROWS + lo, t * ROWS + hi)
            chunk = t * per + b
            mid, before = stats[chunk, 0:1], stats[chunk, 1:2]
            q_mid = query[lo:hi] * emid[at, :]
            q_all = q_mid * jnp.exp(mid)
            qdev[at, :] = (q_all * jnp.exp(before)).astype(bf16)
            scores = dot(q_mid.astype(bf16), kmid[at, :], ((1,), (1,)))
            scores = jnp.where(causal, scores, 0.0).astype(bf16)
            read[at, :] = dot(scores, val[at, :]) + dot(q_all.astype(bf16), old[chunk], ((1,), (1,)))

    with scope("C"):
        for t in range(nb):
            reads(t)

    conv_order = [1, 0] + list(range(2, nb))
    with scope("relayconv"):
        for t in conv_order[:-1]:
            relay_first(1, t)

    incoming[...] = jnp.zeros_like(incoming)

    def hop_z(source, _):
        with scope("zwait"):
            z_arrival(source).wait_recv()
        matrix, log = unpack(zbuf.at[source])
        incoming[...] = incoming[...] * jnp.exp(log) + matrix
        return 0

    with scope("hopz"):
        lax.fori_loop(0, zz, hop_z, 0)

    def hop_y(source, _):
        matrix, log = unpack(ybuf.at[source])
        incoming[...] = incoming[...] * jnp.exp(log) + matrix
        return 0

    lax.fori_loop(0, yy, hop_y, 0)

    def merge(t):
        here = slice(t * ROWS, (t + 1) * ROWS)
        total = read[here, :] + dot(qdev[here, :], incoming[...].astype(bf16), ((1,), (1,)))
        out = rms(total) * sgainv[...] * jax.nn.silu(gate[here, :].astype(f32))
        put(0, t, out.astype(bf16))
        send(0, t)

    with scope("merge"):
        for t in range(nb):
            merge(t)

    with scope("relayconvlast"):
        relay_first(1, conv_order[-1])
    with scope("relayconv2"):
        for t in conv_order[:-1]:
            relay_second(1, t)

    def relay_state(t, _):
        with scope("relaystate"):
            relay_first(0, t)
        return 0

    lax.fori_loop(0, nb, relay_state, 0)
    with scope("relayconv2last"):
        relay_second(1, conv_order[-1])

    with scope("colwait"):
        for kind in range(2):
            own_cols(kind).wait()
            partner_cols_in(kind).wait_recv()
            for r in range(1, ny):
                for j in range(1, tp // 2):
                    share_cols_in(kind, j, r).wait_recv()

    def finish(t, _):
        with scope("finfar"):
            relay_second(0, t)
        with scope("finwait"):
            for kind in range(2):
                for k in range(tp // 2):
                    arrival(kind, t, lax.rem(partner + 2 * k, tp)).wait_recv()
        outv[rows_at(t), :] = dot(mixed[t], cols[...].reshape(2 * tp * GROUP, ncols)).astype(bf16)
        out_copy(t).start()
        return 0

    lax.fori_loop(0, nb, finish, 0)

    def drain(t, _):
        for kind in range(2):
            for copy in own_copies(kind, t) + near_relays(kind, t) + [far_relay(kind, t)]:
                copy.wait_send()
        return 0

    with scope("drain"):
        lax.fori_loop(0, nb, drain, 0)
        for kind in range(2):
            partner_cols(kind).wait_send()
            for k in range(tp - 2):
                far_cols(kind, k).wait_send()
            for r in range(1, ny):
                for j in range(1, tp // 2):
                    share_cols(kind, j, r).wait_send()
        for r in range(1, ny):
            y_copy(r).wait_send()

        def drain_z(target, _):
            z_copy(target).wait_send()
            return 0

        lax.fori_loop(zz + 1, nz, drain_z, 0)

        @pl.when(place < sp - 1)
        def _():
            rim_copy.wait_send()

    with scope("outwait"):
        for t in range(nb):
            out_copy(t).wait()


def body(
    tokens, in_gain, w_query, w_forget, w_input, w_outgate, w_conv_h, w_conv_b, w_conv_c,
    forget_floor, forget_leak, state_gain, conv_taps, group_gain, out_state, out_conv,
):
    count, feats = tokens.shape
    tp, sp = lax.axis_size("tp"), lax.axis_size("sp")
    ny, nz = NY, sp // NY
    ncols, nb = out_state.shape[1] // tp, count // ROWS
    nchunk = count // CHUNK
    hbm, vmem = pl.BlockSpec(memory_space=pl.ANY), pl.BlockSpec(memory_space=pltpu.VMEM)
    sems = pltpu.SemaphoreType.DMA
    return pl.pallas_call(
        functools.partial(fused_kernel, tp, ny, nz),
        in_specs=[hbm] * 16,
        out_specs=hbm,
        out_shape=jax.ShapeDtypeStruct((count, ncols), bf16),
        scratch_shapes=[
            pltpu.VMEM((count, feats), bf16),
            pltpu.VMEM((feats, 7 * GROUP), bf16),
            pltpu.VMEM((count, GROUP), f32),
            pltpu.VMEM((2 * tp, GROUP, ncols), bf16),
            pltpu.VMEM((nb, ROWS, 2 * tp * GROUP), bf16),
            pltpu.VMEM((count, GROUP), bf16),
            pltpu.VMEM((count, GROUP), bf16),
            pltpu.VMEM((count, GROUP), f32),
            pltpu.VMEM((nchunk, GROUP, GROUP), bf16),
            pltpu.VMEM((nchunk, HALO, GROUP), f32),
            pltpu.VMEM((count, GROUP), bf16),
            pltpu.VMEM((count, GROUP), f32),
            pltpu.VMEM((count, GROUP), bf16),
            pltpu.VMEM((count, GROUP), f32),
            pltpu.VMEM((count, ncols), bf16),
            pltpu.VMEM((1, feats), f32),
            pltpu.VMEM((1, GROUP), f32),
            pltpu.VMEM((1, GROUP), f32),
            pltpu.VMEM((1, GROUP), f32),
            pltpu.VMEM((TAPS, GROUP), bf16),
            pltpu.VMEM((HALO + count, GROUP), f32),
            pltpu.VMEM((GROUP, GROUP), f32),
            pltpu.VMEM((ny, GROUP + LOGS, GROUP), bf16),
            pltpu.VMEM((nz, GROUP + LOGS, GROUP), bf16),
            pltpu.VMEM((HALO, GROUP), f32),
            pltpu.VMEM((HALO, GROUP), f32),
            pltpu.VMEM((2 * HALO, GROUP), f32),
            sems((nb,)), sems((7,)), sems((6,)), sems((2,)), sems((nb,)),
            pltpu.SemaphoreType.REGULAR((1,)), pltpu.SemaphoreType.REGULAR((1,)),
            sems((2, tp)), sems((2, tp)), sems((2, tp // 2, ny)), sems((2, tp // 2, ny)),
            sems((ny,)), sems((ny,)), sems((nz,)), sems((nz,)), sems((1,)), sems((1,)),
            sems((2, 7, nb)), sems((2, tp, nb)),
        ],
        compiler_params=pltpu.CompilerParams(
            vmem_limit_bytes=67043328, collective_id=0, has_side_effects=True
        ),
    )(
        tokens, in_gain[None], w_query, w_forget, w_input, w_outgate, w_conv_h, w_conv_b, w_conv_c,
        forget_floor[None], forget_leak, state_gain[None], conv_taps, group_gain[None],
        out_state, out_conv,
    )


def solution(mesh):
    cols, rows = P(None, "tp"), P("tp", None)
    in_specs = (
        P("sp", None), P(), cols, cols, cols, cols, cols, cols, cols,
        P("tp"), P("sp", "tp"), P(), cols, P(), rows, rows,
    )
    return jax.shard_map(
        body, mesh=mesh, in_specs=in_specs, out_specs=P("sp", "tp"), check_vma=False
    )
```

```python
import functools

import jax
import jax.numpy as jnp
from jax import lax
from jax.experimental import pallas as pl
from jax.experimental.pallas import tpu as pltpu
from jax.sharding import PartitionSpec as P

GROUP = 128
CHUNK = 128
ROWS = 256
TAPS = 3
HALO = 8
NY = 4
LOGS = 16
STRIP = 16

norm_eps = 1e-06
f32 = jnp.float32
bf16 = jnp.bfloat16


scope = jax.named_scope


def dot(a, b, dims=((1,), (0,))):
    return lax.dot_general(a, b, (dims, ((), ())), preferred_element_type=f32)


def rms(values):
    return values * lax.rsqrt(jnp.mean(values * values, axis=-1, keepdims=True) + norm_eps)


def split(values):
    hi = values.astype(bf16)
    return hi, (values - hi.astype(f32)).astype(bf16)


def fused_kernel(
    tp, ny, nz,
    tokens, in_gain, wq, wf, wi, wg, wh, wb, wc, floor, leak, state_gain, taps, group_gain,
    out_state, out_conv, result,
    tok, w, leakv, cols, mixed, xs, kmid, val, emid, old, stats, gate, read, qdev, scl, acc,
    gainv, floorv, sgainv, ggainv, tapsv, prods, wide,
    pad, incoming, ybuf, zbuf, rim, tail,
    tok_sem, w_sem, small_sem, own_sem, ready_z, ready_rim,
    colx_send, colx_recv, coly_send, coly_recv,
    y_send, y_recv, z_send, z_recv, rim_send, rim_recv, blk_send, near_recv, far_recv, pair_recv,
):
    me, place = lax.axis_index("tp"), lax.axis_index("sp")
    sp = ny * nz
    core, chip = lax.rem(me, 2), lax.div(me, 2)
    partner = me + 1 - 2 * core
    yy, zz = lax.rem(place, ny), lax.div(place, ny)
    far = lax.rem(me + 4, tp)
    ahead = lax.rem(me + tp + 2 - 4 * core, tp)
    behind = lax.rem(me + tp - 2 + 4 * core, tp)
    y_ahead = lax.rem(yy + ny + 1 - 2 * core, ny)
    y_behind = lax.rem(yy + ny - 1 + 2 * core, ny)
    count, ncols = result.shape
    nb = count // ROWS
    nchunk = count // CHUNK
    part = GROUP // ny
    per = ROWS // CHUNK
    outs = (out_state, out_conv)

    def rows_at(t):
        return pl.ds(pl.multiple_of(t * ROWS, ROWS), ROWS)

    def tok_copy(t):
        return pltpu.make_async_copy(tokens.at[rows_at(t)], tok.at[rows_at(t)], tok_sem.at[t])

    weights = (wf, wi, wc, wh, wb, wg, wq)

    def w_copy(i):
        return pltpu.make_async_copy(
            weights[i], w.at[:, i * GROUP : (i + 1) * GROUP], w_sem.at[i // 2]
        )

    def w_wait(first, last):
        ref = w.at[:, first * GROUP : last * GROUP]
        pltpu.make_async_copy(ref, ref, w_sem.at[first // 2]).wait()

    smalls = (
        pltpu.make_async_copy(in_gain, gainv, small_sem.at[0]),
        pltpu.make_async_copy(floor, floorv, small_sem.at[1]),
        pltpu.make_async_copy(leak, leakv, small_sem.at[2]),
        pltpu.make_async_copy(taps, tapsv, small_sem.at[3]),
        pltpu.make_async_copy(group_gain, ggainv, small_sem.at[4]),
        pltpu.make_async_copy(state_gain, sgainv, small_sem.at[5]),
    )

    def col_slice(target):
        return pl.ds(pl.multiple_of(target * ncols, ncols), ncols)

    mine_rows = pl.ds(pl.multiple_of(yy * part, part), part)

    def landed(ref, send, recv):
        return pltpu.make_async_remote_copy(ref, ref, send, recv, device_id={"tp": partner})

    def own_cols(kind):
        return pltpu.make_async_copy(
            outs[kind].at[:, col_slice(me)], cols.at[kind * tp + me], own_sem.at[0]
        )

    own_cols_done = pltpu.make_async_copy(
        cols.at[pl.ds(0, 2)], cols.at[pl.ds(0, 2)], own_sem.at[0]
    )

    def partner_cols(kind):
        return pltpu.make_async_remote_copy(
            outs[kind].at[:, col_slice(partner)], cols.at[kind * tp + me],
            colx_send.at[0], colx_recv.at[1], device_id={"tp": partner},
        )

    def far_cols(kind, k):
        target = lax.rem(2 * chip + 2 + k, tp)
        return pltpu.make_async_remote_copy(
            outs[kind].at[mine_rows, col_slice(target)], cols.at[kind * tp + me, mine_rows],
            colx_send.at[0], colx_recv.at[0], device_id={"tp": target},
        )

    far_units = 2 * (tp - 2) // ny
    far_cols_in = landed(cols.at[pl.ds(0, far_units)], colx_send.at[0], colx_recv.at[0])
    partner_cols_in = landed(cols.at[pl.ds(0, 2)], colx_send.at[0], colx_recv.at[1])
    colx_sent = landed(cols.at[pl.ds(0, far_units + 2)], colx_send.at[0], colx_recv.at[0])

    def share_cols(kind, j, origin, target, slot):
        pair = pl.ds(kind * tp + lax.rem(2 * chip + 2 * j, tp), 2)
        ref = cols.at[pair, pl.ds(pl.multiple_of(origin * part, part), part)]
        return pltpu.make_async_remote_copy(
            ref, ref, coly_send.at[0], coly_recv.at[slot], device_id={"sp": zz * ny + target}
        )

    def share_all(origin, target, slot):
        for kind in range(2):
            for j in range(1, tp // 2):
                share_cols(kind, j, origin, target, slot).start()

    def shared_in(slot):
        return landed(cols.at[pl.ds(0, far_units)], coly_send.at[0], coly_recv.at[slot])

    shares_sent = landed(cols.at[pl.ds(0, 3 * far_units)], coly_send.at[0], coly_recv.at[0])

    def y_copy(r):
        ref = ybuf.at[yy]
        return pltpu.make_async_remote_copy(
            ref, ref, y_send.at[0], y_recv.at[0],
            device_id={"sp": zz * ny + lax.rem(yy + r, ny)},
        )

    y_all = landed(ybuf.at[pl.ds(0, ny - 1)], y_send.at[0], y_recv.at[0])

    def z_copy(target):
        ref = zbuf.at[zz]
        return pltpu.make_async_remote_copy(
            ref, ref, z_send.at[target], z_recv.at[zz], device_id={"sp": target * ny + yy}
        )

    def z_arrival(source):
        ref = zbuf.at[source]
        return pltpu.make_async_remote_copy(
            ref, ref, z_send.at[source], z_recv.at[source], device_id={"sp": source * ny + yy}
        )

    rim_copy = pltpu.make_async_remote_copy(
        tail, rim, rim_send.at[0], rim_recv.at[0], device_id={"sp": place + 1}
    )
    rim_arrival = pltpu.make_async_remote_copy(
        tail, rim, rim_send.at[0], rim_recv.at[0], device_id={"sp": place - 1}
    )

    def block_copy(kind, t, origin, target, recv):
        lanes = pl.ds(pl.multiple_of((kind * tp + origin) * GROUP, GROUP), GROUP)
        ref = mixed.at[t, :, lanes]
        return pltpu.make_async_remote_copy(
            ref, ref, blk_send.at[0], recv.at[kind, t], device_id={"tp": target}
        )

    def relay_first(kind, t):
        landed(mixed.at[t, :, 0 : 2 * GROUP], blk_send.at[0], near_recv.at[kind, t]).wait_recv()
        block_copy(kind, t, behind, ahead, far_recv).start()
        block_copy(kind, t, behind, partner, pair_recv).start()
        block_copy(kind, t, ahead, partner, pair_recv).start()

    def relay_second(kind, t):
        landed(mixed.at[t, :, 0:GROUP], blk_send.at[0], far_recv.at[kind, t]).wait_recv()
        block_copy(kind, t, far, partner, pair_recv).start()

    def pair_wait(kind, t):
        half = mixed.at[t, :, 0 : tp // 2 * GROUP]
        landed(half, blk_send.at[0], pair_recv.at[kind, t]).wait_recv()

    blocks_sent = landed(
        mixed.at[:, :, 0 : 2 * (tp - 1) * GROUP], blk_send.at[0], pair_recv.at[0, 0]
    )

    def put(kind, t, value):
        lanes = pl.ds(pl.multiple_of((kind * tp + me) * GROUP, GROUP), GROUP)
        mixed[t, :, lanes] = value

    smalls[0].start()
    tok_copy(0).start()
    w_copy(0).start()
    w_copy(1).start()
    smalls[1].start()
    barrier = pltpu.get_barrier_semaphore()
    for k in range(1, tp):
        pl.semaphore_signal(barrier, inc=1, device_id={"tp": lax.rem(me + k, tp)})
    for r in range(1, ny):
        pl.semaphore_signal(barrier, inc=1, device_id={"sp": zz * ny + lax.rem(yy + r, ny)})

    def greet_z(target, _):
        pl.semaphore_signal(barrier, inc=1, device_id={"sp": target * ny + yy})
        return 0

    lax.fori_loop(zz + 1, nz, greet_z, 0)

    @pl.when(jnp.logical_and(yy == ny - 1, zz < nz - 1))
    def _():
        pl.semaphore_signal(barrier, inc=1, device_id={"sp": place + 1})

    def meet():
        with scope("barrier"):
            across = jnp.where(yy == 0, jnp.minimum(zz, 1), 0)
            pl.semaphore_wait(barrier, tp + ny - 2 + zz + across)

        def ready(target, _):
            pl.semaphore_signal(ready_z.at[0], inc=1, device_id={"sp": target * ny + yy})
            return 0

        lax.fori_loop(0, zz, ready, 0)

        @pl.when(jnp.logical_and(yy == 0, zz > 0))
        def _():
            pl.semaphore_signal(ready_rim.at[0], inc=1, device_id={"sp": place - 1})

        for kind in range(2):
            for k in range(tp - 2):
                far_cols(kind, k).start()
        for kind in range(2):
            partner_cols(kind).start()
            own_cols(kind).start()

    row = lax.broadcasted_iota(jnp.int32, (CHUNK, CHUNK), 0)
    col = lax.broadcasted_iota(jnp.int32, (CHUNK, CHUNK), 1)
    causal = row >= col
    ones = causal.astype(bf16)

    def lanes(first, last):
        return slice(first * GROUP, last * GROUP)

    def span(t):
        return slice(t * ROWS, (t + 1) * ROWS)

    def prepare(t):
        gain = gainv[...].astype(bf16)
        for r in range(t * ROWS, (t + 1) * ROWS, STRIP):
            raw = tok[r : r + STRIP, :]
            feats = raw.shape[1]
            tok[r : r + STRIP, :] = raw * gain
            squares = raw * raw
            squares = squares[:, : feats // 2] + squares[:, feats // 2 :]
            squares = squares[:, : feats // 4] + squares[:, feats // 4 :]
            mean = jnp.sum(squares.astype(f32), axis=1, keepdims=True) * (1.0 / feats)
            scl[r : r + STRIP, :] = jnp.broadcast_to(lax.rsqrt(mean + norm_eps), (STRIP, GROUP))

    def project_states(t):
        here = span(t)
        both = dot(tok[here, :], w[:, lanes(0, 2)])
        scale = scl[here, :]
        xs[here, :] = (both[:, :GROUP] * scale).astype(bf16)
        val[here, :] = (both[:, GROUP:] * scale).astype(bf16)

    def chain(t, carry):
        state, offset = carry
        here = span(t)
        key = (1.0 - floorv[...]) * jax.nn.sigmoid(-xs[here, :].astype(f32))
        terms = split(jnp.log(1.0 - key) + leakv[here, :])
        cums = []
        for b in range(per):
            rows = slice(b * CHUNK, (b + 1) * CHUNK)
            sums = dot(ones, jnp.concatenate([term[rows] for term in terms], axis=1))
            cums.append(sums[:, :GROUP] + sums[:, GROUP:])
        fresh = []
        for b in range(per):
            chunk, cum = t * per + b, cums[b]
            at = slice(chunk * CHUNK, (chunk + 1) * CHUNK)
            mid = cum[CHUNK // 2 - 1 : CHUNK // 2]
            last = cum[CHUNK - 1 : CHUNK]
            emid[at, :] = jnp.exp(cum - mid)
            k_mid = key[b * CHUNK : (b + 1) * CHUNK] * jnp.exp(mid - cum)
            kmid[at, :] = k_mid.astype(bf16)
            k_end = (k_mid * jnp.exp(last - mid)).astype(bf16)
            stats[chunk, 0:1] = mid
            fresh.append(dot(val[at, :], k_end, ((0,), (0,))))
        for b in range(per):
            chunk, last = t * per + b, cums[b][CHUNK - 1 : CHUNK]
            old[chunk] = state.astype(bf16)
            stats[chunk, 1:2] = offset
            state = state * jnp.exp(last) + fresh[b]
            offset = offset + last
        return state, offset

    def gated_inputs(both, factor):
        left = (both[:, :GROUP] * factor).astype(bf16).astype(f32)
        right = (both[:, GROUP:] * factor).astype(bf16).astype(f32)
        return (left * right).astype(bf16).astype(f32)

    carry = (jnp.zeros((GROUP, GROUP), f32), jnp.zeros((1, GROUP), f32))
    with scope("load0"):
        smalls[0].wait()
        tok_copy(0).wait()
    smalls[2].start()
    for t in range(1, nb):
        tok_copy(t).start()
    for i in range(2, 7):
        w_copy(i).start()
    for copy in smalls[3:]:
        copy.start()
    with scope("prep0"):
        prepare(0)
    with scope("load1"):
        w_wait(0, 2)
        smalls[1].wait()
    with scope("A"):
        project_states(0)
        smalls[2].wait()
        for t in range(1, nb):
            with scope("tokwait"):
                tok_copy(t).wait()
            prepare(t)
            carry = chain(t - 1, carry)
            project_states(t)
            if t == 1:
                meet()

    with scope("w23wait"):
        w_wait(2, 4)
    with scope("rimsend"):
        end = slice(count - 2 * HALO, count)
        tail[...] = gated_inputs(dot(tok[end, :], w[:, lanes(2, 4)]), scl[end, :])[HALO:]

        @pl.when(jnp.logical_and(yy == ny - 1, zz < nz - 1))
        def _():
            pl.semaphore_wait(ready_rim.at[0], 1)

        @pl.when(place < sp - 1)
        def _():
            rim_copy.start()

    with scope("A2"):
        carry = chain(nb - 1, carry)

    def pack(slot, matrix, logs):
        hi = logs.astype(bf16)
        mid, low = split(logs - hi.astype(f32))
        slot[0:GROUP, :] = matrix.astype(bf16)
        r = lax.broadcasted_iota(jnp.int32, (LOGS, GROUP), 0)
        rows = jnp.where(r == 0, hi.astype(f32), jnp.where(r == 1, mid.astype(f32), low.astype(f32)))
        slot[GROUP : GROUP + LOGS, :] = rows.astype(bf16)

    def unpack(slot):
        logs = slot[GROUP : GROUP + LOGS, :].astype(f32)
        return slot[0:GROUP, :].astype(f32), logs[0:1] + logs[1:2] + logs[2:3]

    pack(ybuf.at[yy], *carry)
    for r in range(1, ny):
        y_copy(r).start()

    with scope("w46wait"):
        w_wait(4, 6)
        w_wait(6, 7)
        for copy in smalls[3:]:
            copy.wait()
    taps_f = tapsv[...].astype(f32)
    pad[0:HALO, :] = jnp.zeros((HALO, GROUP), f32)

    def convolve(first, size, conv_in, proj_b):
        total = taps_f[TAPS - 1 : TAPS] * conv_in
        for j in range(TAPS - 1):
            start = HALO - (TAPS - 1) + j + first
            total += taps_f[j : j + 1] * pad[start : start + size, :]
        return (rms(proj_b * total) * ggainv[...]).astype(bf16)

    def project_inputs(t):
        here = span(t)
        pad[HALO + t * ROWS : HALO + (t + 1) * ROWS, :] = gated_inputs(
            dot(tok[here, :], w[:, lanes(2, 4)]), scl[here, :]
        )

    def project_gates(t):
        here = span(t)
        both = dot(tok[here, :], w[:, lanes(4, 6)])
        factor = scl[here, :]
        prods[here, :] = (both[:, :GROUP] * factor).astype(bf16)
        gate[here, :] = (both[:, GROUP:] * factor).astype(bf16)

    def project_query(t):
        here = span(t)
        wide[here, :] = (dot(tok[here, :], w[:, lanes(6, 7)]) * scl[here, :]).astype(bf16)

    def send(kind, t):
        block_copy(kind, t, me, ahead, near_recv).start()
        block_copy(kind, t, me, behind, near_recv).start()
        block_copy(kind, t, me, partner, pair_recv).start()

    def conv(t):
        conv_in = pad[HALO + t * ROWS : HALO + (t + 1) * ROWS, :]
        put(1, t, convolve(t * ROWS, ROWS, conv_in, prods[span(t), :].astype(f32)))

    def reads(chunk):
        at = slice(chunk * CHUNK, (chunk + 1) * CHUNK)
        query = jax.nn.silu(wide[at, :].astype(f32))
        mid, before = stats[chunk, 0:1], stats[chunk, 1:2]
        q_mid = query * emid[at, :]
        q_all = q_mid * jnp.exp(mid)
        qdev[at, :] = (q_all * jnp.exp(before)).astype(bf16)
        scores = dot(q_mid.astype(bf16), kmid[at, :], ((1,), (1,)))
        scores = jnp.where(causal, scores, 0.0).astype(bf16)
        read[at, :] = dot(scores, val[at, :]) + dot(q_all.astype(bf16), old[chunk], ((1,), (1,)))

    def combine():
        with scope("ywait"):
            y_all.wait_recv()
        whole, logs = unpack(ybuf.at[0])
        for j in range(1, ny):
            more, log = unpack(ybuf.at[j])
            whole = whole * jnp.exp(log) + more
            logs = logs + log
        pack(zbuf.at[zz], whole, logs)
        with scope("readyz"):
            @pl.when(zz < nz - 1)
            def _():
                pl.semaphore_wait(ready_z.at[0], nz - 1 - zz)

        def send_z(target, _):
            z_copy(target).start()
            return 0

        lax.fori_loop(zz + 1, nz, send_z, 0)

    def first_rows():
        with scope("rimwait"):
            @pl.when(place > 0)
            def _():
                rim_arrival.wait_recv()
                pad[0:HALO, :] = rim[...]

        conv(0)
        send(1, 0)

    def share():
        with scope("colxwait"):
            far_cols_in.wait_recv()
        share_all(yy, y_ahead, 0)
        share_all(yy, y_behind, 1)

    def share_on():
        with scope("colywait"):
            shared_in(0).wait_recv()
        share_all(y_behind, y_ahead, 2)

    with scope("B"):
        project_inputs(0)
        project_inputs(1)
        project_gates(1)
        conv(1)
        send(1, 1)
        project_gates(0)
        first_rows()
    share()
    combine()
    with scope("B2"):
        project_inputs(2)
        project_gates(2)
        conv(2)
        project_query(0)
        send(1, 2)
    with scope("B3"):
        project_inputs(3)
        project_gates(3)
        conv(3)
        project_query(1)
        reads(0)
        reads(1)
        send(1, 3)
    with scope("C2"):
        project_query(2)
        reads(2)
        reads(3)
        project_query(3)
        reads(4)
        reads(5)
    with scope("C3"):
        reads(6)
        reads(7)

    share_on()
    conv_order = [1, 0] + list(range(2, nb))
    with scope("relayconv"):
        for t in conv_order[:-1]:
            relay_first(1, t)

    incoming[...] = jnp.zeros_like(incoming)

    def hop_z(source, _):
        z_arrival(source).wait_recv()
        matrix, log = unpack(zbuf.at[source])
        incoming[...] = incoming[...] * jnp.exp(log) + matrix
        return 0

    with scope("hopz"):
        lax.fori_loop(0, zz, hop_z, 0)

    def hop_y(source, _):
        matrix, log = unpack(ybuf.at[source])
        incoming[...] = incoming[...] * jnp.exp(log) + matrix
        return 0

    lax.fori_loop(0, yy, hop_y, 0)

    def merge(t):
        here = span(t)
        total = read[here, :] + dot(qdev[here, :], incoming[...].astype(bf16), ((1,), (1,)))
        out = rms(total) * sgainv[...] * jax.nn.silu(gate[here, :].astype(f32))
        put(0, t, out.astype(bf16))
        send(0, t)

    with scope("merge"):
        for t in range(nb):
            merge(t)

    def conv_dot(t):
        with scope("convdot"):
            pair_wait(1, t)
            side = cols[tp : 2 * tp].reshape(tp * GROUP, ncols)
            acc[span(t), :] = dot(mixed[t, :, tp * GROUP :], side)

    with scope("relayconvlast"):
        relay_first(1, conv_order[-1])
    for t in range(nb - 1):
        with scope("relaystate"):
            relay_first(0, t)
        with scope("relayconv2"):
            relay_second(1, conv_order[t])
    with scope("colwait"):
        own_cols_done.wait()
        partner_cols_in.wait_recv()
        shared_in(1).wait_recv()
        shared_in(2).wait_recv()
    for t in conv_order[:-1]:
        conv_dot(t)
    with scope("relaystate"):
        relay_first(0, nb - 1)
    with scope("relayconv2last"):
        relay_second(1, conv_order[-1])

    def finish(t):
        with scope("finwait"):
            pair_wait(0, t)
        with scope("findot"):
            total = acc[span(t), :] + dot(mixed[t, :, : tp * GROUP], cols[0:tp].reshape(tp * GROUP, ncols))
            result[span(t), :] = total.astype(bf16)

    for t in range(nb):
        with scope("finfar"):
            relay_second(0, t)
        if t == 0:
            conv_dot(conv_order[-1])
        else:
            finish(t - 1)
    finish(nb - 1)

    with scope("drain"):
        blocks_sent.wait_send()
        colx_sent.wait_send()
        shares_sent.wait_send()
        y_all.wait_send()

        def drain_z(target, _):
            z_copy(target).wait_send()
            return 0

        lax.fori_loop(zz + 1, nz, drain_z, 0)

        @pl.when(place < sp - 1)
        def _():
            rim_copy.wait_send()


def body(
    tokens, in_gain, w_query, w_forget, w_input, w_outgate, w_conv_h, w_conv_b, w_conv_c,
    forget_floor, forget_leak, state_gain, conv_taps, group_gain, out_state, out_conv,
):
    count, feats = tokens.shape
    tp, sp = lax.axis_size("tp"), lax.axis_size("sp")
    ny, nz = NY, sp // NY
    ncols, nb = out_state.shape[1] // tp, count // ROWS
    nchunk = count // CHUNK
    hbm, vmem = pl.BlockSpec(memory_space=pltpu.HBM), pl.BlockSpec(memory_space=pltpu.VMEM)
    sems = pltpu.SemaphoreType.DMA
    return pl.pallas_call(
        functools.partial(fused_kernel, tp, ny, nz),
        in_specs=[hbm] * 16,
        out_specs=vmem,
        out_shape=jax.ShapeDtypeStruct((count, ncols), bf16),
        scratch_shapes=[
            pltpu.VMEM((count, feats), bf16),
            pltpu.VMEM((feats, 7 * GROUP), bf16),
            pltpu.VMEM((count, GROUP), f32),
            pltpu.VMEM((2 * tp, GROUP, ncols), bf16),
            pltpu.VMEM((nb, ROWS, 2 * tp * GROUP), bf16),
            pltpu.VMEM((count, GROUP), bf16),
            pltpu.VMEM((count, GROUP), bf16),
            pltpu.VMEM((count, GROUP), bf16),
            pltpu.VMEM((count, GROUP), f32),
            pltpu.VMEM((nchunk, GROUP, GROUP), bf16),
            pltpu.VMEM((nchunk, HALO, GROUP), f32),
            pltpu.VMEM((count, GROUP), bf16),
            pltpu.VMEM((count, GROUP), f32),
            pltpu.VMEM((count, GROUP), bf16),
            pltpu.VMEM((count, GROUP), f32),
            pltpu.VMEM((count, ncols), f32),
            pltpu.VMEM((1, feats), f32),
            pltpu.VMEM((1, GROUP), f32),
            pltpu.VMEM((1, GROUP), f32),
            pltpu.VMEM((1, GROUP), f32),
            pltpu.VMEM((TAPS, GROUP), bf16),
            pltpu.VMEM((count, GROUP), bf16),
            pltpu.VMEM((count, GROUP), bf16),
            pltpu.VMEM((HALO + count, GROUP), f32),
            pltpu.VMEM((GROUP, GROUP), f32),
            pltpu.VMEM((ny, GROUP + LOGS, GROUP), bf16),
            pltpu.VMEM((nz, GROUP + LOGS, GROUP), bf16),
            pltpu.VMEM((HALO, GROUP), f32),
            pltpu.VMEM((HALO, GROUP), f32),
            sems((nb,)), sems((4,)), sems((6,)), sems((1,)),
            pltpu.SemaphoreType.REGULAR((1,)), pltpu.SemaphoreType.REGULAR((1,)),
            sems((1,)), sems((2,)), sems((1,)), sems((3,)),
            sems((1,)), sems((1,)), sems((nz,)), sems((nz,)), sems((1,)), sems((1,)),
            sems((1,)), sems((2, nb)), sems((2, nb)), sems((2, nb)),
        ],
        compiler_params=pltpu.CompilerParams(
            vmem_limit_bytes=40 * 2**20, collective_id=0, has_side_effects=True
        ),
    )(*[pltpu.with_memory_space_constraint(a, pltpu.HBM) for a in (
        tokens, in_gain[None], w_query, w_forget, w_input, w_outgate, w_conv_h, w_conv_b, w_conv_c,
        forget_floor[None], forget_leak, state_gain[None], conv_taps, group_gain[None],
        out_state, out_conv,
    )])


def solution(mesh):
    cols, rows = P(None, "tp"), P("tp", None)
    in_specs = (
        P("sp", None), P(), cols, cols, cols, cols, cols, cols, cols,
        P("tp"), P("sp", "tp"), P(), cols, P(), rows, rows,
    )
    return jax.shard_map(
        body, mesh=mesh, in_specs=in_specs, out_specs=P("sp", "tp"), check_vma=False
    )
```

```python
import functools

import jax
import jax.numpy as jnp
from jax import lax
from jax.experimental import pallas as pl
from jax.experimental.pallas import tpu as pltpu
from jax.sharding import PartitionSpec as P

GROUP = 128
CHUNK = 128
ROWS = 256
TAPS = 3
HALO = 8
NY = 4
LOGS = 16
STRIP = 16

norm_eps = 1e-06
f32 = jnp.float32
bf16 = jnp.bfloat16


scope = jax.named_scope


def dot(a, b, dims=((1,), (0,))):
    return lax.dot_general(a, b, (dims, ((), ())), preferred_element_type=f32)


def rms(values):
    return values * lax.rsqrt(jnp.mean(values * values, axis=-1, keepdims=True) + norm_eps)


def split(values):
    hi = values.astype(bf16)
    return hi, (values - hi.astype(f32)).astype(bf16)


def fused_kernel(
    tp, ny, nz,
    tokens, in_gain, wq, wf, wi, wg, wh, wb, wc, floor, leak, state_gain, taps, group_gain,
    out_state, out_conv, result,
    tok, w, leakv, cols, mixed, xs, kmid, val, emid, old, stats, gate, read, qdev, scl, acc,
    gainv, floorv, sgainv, ggainv, tapsv, prods, wide, keyv, terms, kend,
    pad, incoming, ybuf, zbuf, rim, tail,
    tok_sem, w_sem, small_sem, own_sem, ready_z, ready_rim,
    colx_send, colx_recv, coly_send, coly_recv,
    y_send, y_recv, z_send, z_recv, rim_send, rim_recv, blk_send, near_recv, far_recv, pair_recv,
):
    me, place = lax.axis_index("tp"), lax.axis_index("sp")
    sp = ny * nz
    core, chip = lax.rem(me, 2), lax.div(me, 2)
    partner = me + 1 - 2 * core
    yy, zz = lax.rem(place, ny), lax.div(place, ny)
    far = lax.rem(me + 4, tp)
    ahead = lax.rem(me + tp + 2 - 4 * core, tp)
    behind = lax.rem(me + tp - 2 + 4 * core, tp)
    y_ahead = lax.rem(yy + ny + 1 - 2 * core, ny)
    y_behind = lax.rem(yy + ny - 1 + 2 * core, ny)
    count, ncols = result.shape
    nb = count // ROWS
    nchunk = count // CHUNK
    part = GROUP // ny
    per = ROWS // CHUNK
    outs = (out_state, out_conv)

    def rows_at(t):
        return pl.ds(pl.multiple_of(t * ROWS, ROWS), ROWS)

    def tok_copy(t):
        return pltpu.make_async_copy(tokens.at[rows_at(t)], tok.at[rows_at(t)], tok_sem.at[t])

    weights = (wf, wi, wc, wh, wb, wg, wq)

    def w_copy(i):
        return pltpu.make_async_copy(
            weights[i], w.at[:, i * GROUP : (i + 1) * GROUP], w_sem.at[i // 2]
        )

    def w_wait(first, last):
        ref = w.at[:, first * GROUP : last * GROUP]
        pltpu.make_async_copy(ref, ref, w_sem.at[first // 2]).wait()

    smalls = (
        pltpu.make_async_copy(in_gain, gainv, small_sem.at[0]),
        pltpu.make_async_copy(floor, floorv, small_sem.at[1]),
        pltpu.make_async_copy(leak, leakv, small_sem.at[2]),
        pltpu.make_async_copy(taps, tapsv, small_sem.at[3]),
        pltpu.make_async_copy(group_gain, ggainv, small_sem.at[4]),
        pltpu.make_async_copy(state_gain, sgainv, small_sem.at[5]),
    )

    def col_slice(target):
        return pl.ds(pl.multiple_of(target * ncols, ncols), ncols)

    mine_rows = pl.ds(pl.multiple_of(yy * part, part), part)

    def landed(ref, send, recv):
        return pltpu.make_async_remote_copy(ref, ref, send, recv, device_id={"tp": partner})

    def own_cols(kind):
        return pltpu.make_async_copy(
            outs[kind].at[:, col_slice(me)], cols.at[kind * tp + me], own_sem.at[0]
        )

    own_cols_done = pltpu.make_async_copy(
        cols.at[pl.ds(0, 2)], cols.at[pl.ds(0, 2)], own_sem.at[0]
    )

    def partner_cols(kind):
        return pltpu.make_async_remote_copy(
            outs[kind].at[:, col_slice(partner)], cols.at[kind * tp + me],
            colx_send.at[0], colx_recv.at[1], device_id={"tp": partner},
        )

    def far_cols(kind, k):
        target = lax.rem(2 * chip + 2 + k, tp)
        return pltpu.make_async_remote_copy(
            outs[kind].at[mine_rows, col_slice(target)], cols.at[kind * tp + me, mine_rows],
            colx_send.at[0], colx_recv.at[0], device_id={"tp": target},
        )

    far_units = 2 * (tp - 2) // ny
    far_cols_in = landed(cols.at[pl.ds(0, far_units)], colx_send.at[0], colx_recv.at[0])
    partner_cols_in = landed(cols.at[pl.ds(0, 2)], colx_send.at[0], colx_recv.at[1])
    colx_sent = landed(cols.at[pl.ds(0, far_units + 2)], colx_send.at[0], colx_recv.at[0])

    def share_cols(kind, j, origin, target, slot):
        pair = pl.ds(kind * tp + lax.rem(2 * chip + 2 * j, tp), 2)
        ref = cols.at[pair, pl.ds(pl.multiple_of(origin * part, part), part)]
        return pltpu.make_async_remote_copy(
            ref, ref, coly_send.at[0], coly_recv.at[slot], device_id={"sp": zz * ny + target}
        )

    def share_all(origin, target, slot):
        for kind in range(2):
            for j in range(1, tp // 2):
                share_cols(kind, j, origin, target, slot).start()

    def shared_in(slot):
        return landed(cols.at[pl.ds(0, far_units)], coly_send.at[0], coly_recv.at[slot])

    shares_sent = landed(cols.at[pl.ds(0, 3 * far_units)], coly_send.at[0], coly_recv.at[0])

    def y_copy(r):
        ref = ybuf.at[yy]
        return pltpu.make_async_remote_copy(
            ref, ref, y_send.at[0], y_recv.at[0],
            device_id={"sp": zz * ny + lax.rem(yy + r, ny)},
        )

    y_all = landed(ybuf.at[pl.ds(0, ny - 1)], y_send.at[0], y_recv.at[0])

    def z_copy(target):
        ref = zbuf.at[zz]
        return pltpu.make_async_remote_copy(
            ref, ref, z_send.at[target], z_recv.at[zz], device_id={"sp": target * ny + yy}
        )

    def z_arrival(source):
        ref = zbuf.at[source]
        return pltpu.make_async_remote_copy(
            ref, ref, z_send.at[source], z_recv.at[source], device_id={"sp": source * ny + yy}
        )

    rim_copy = pltpu.make_async_remote_copy(
        tail, rim, rim_send.at[0], rim_recv.at[0], device_id={"sp": place + 1}
    )
    rim_arrival = pltpu.make_async_remote_copy(
        tail, rim, rim_send.at[0], rim_recv.at[0], device_id={"sp": place - 1}
    )

    def block_copy(kind, t, origin, target, recv):
        lanes = pl.ds(pl.multiple_of((kind * tp + origin) * GROUP, GROUP), GROUP)
        ref = mixed.at[t, :, lanes]
        return pltpu.make_async_remote_copy(
            ref, ref, blk_send.at[0], recv.at[kind, t], device_id={"tp": target}
        )

    def relay_first(kind, t):
        landed(mixed.at[t, :, 0 : 2 * GROUP], blk_send.at[0], near_recv.at[kind, t]).wait_recv()
        block_copy(kind, t, behind, ahead, far_recv).start()
        block_copy(kind, t, behind, partner, pair_recv).start()
        block_copy(kind, t, ahead, partner, pair_recv).start()

    def relay_second(kind, t):
        landed(mixed.at[t, :, 0:GROUP], blk_send.at[0], far_recv.at[kind, t]).wait_recv()
        block_copy(kind, t, far, partner, pair_recv).start()

    def pair_wait(kind, t):
        half = mixed.at[t, :, 0 : tp // 2 * GROUP]
        landed(half, blk_send.at[0], pair_recv.at[kind, t]).wait_recv()

    blocks_sent = landed(
        mixed.at[:, :, 0 : 2 * (tp - 1) * GROUP], blk_send.at[0], pair_recv.at[0, 0]
    )

    def put(kind, t, value):
        lanes = pl.ds(pl.multiple_of((kind * tp + me) * GROUP, GROUP), GROUP)
        mixed[t, :, lanes] = value

    smalls[0].start()
    tok_copy(0).start()
    w_copy(0).start()
    w_copy(1).start()
    smalls[1].start()
    barrier = pltpu.get_barrier_semaphore()
    for k in range(1, tp):
        pl.semaphore_signal(barrier, inc=1, device_id={"tp": lax.rem(me + k, tp)})
    for r in range(1, ny):
        pl.semaphore_signal(barrier, inc=1, device_id={"sp": zz * ny + lax.rem(yy + r, ny)})

    def greet_z(target, _):
        pl.semaphore_signal(barrier, inc=1, device_id={"sp": target * ny + yy})
        return 0

    lax.fori_loop(zz + 1, nz, greet_z, 0)

    @pl.when(jnp.logical_and(yy == ny - 1, zz < nz - 1))
    def _():
        pl.semaphore_signal(barrier, inc=1, device_id={"sp": place + 1})

    for t in range(1, nb):
        tok_copy(t).start()
    smalls[2].start()

    def meet():
        with scope("barrier"):
            across = jnp.where(yy == 0, jnp.minimum(zz, 1), 0)
            pl.semaphore_wait(barrier, tp + ny - 2 + zz + across)

        def ready(target, _):
            pl.semaphore_signal(ready_z.at[0], inc=1, device_id={"sp": target * ny + yy})
            return 0

        lax.fori_loop(0, zz, ready, 0)

        @pl.when(jnp.logical_and(yy == 0, zz > 0))
        def _():
            pl.semaphore_signal(ready_rim.at[0], inc=1, device_id={"sp": place - 1})

        for kind in range(2):
            for k in range(tp - 2):
                far_cols(kind, k).start()
        for kind in range(2):
            partner_cols(kind).start()
            own_cols(kind).start()

    row = lax.broadcasted_iota(jnp.int32, (CHUNK, CHUNK), 0)
    col = lax.broadcasted_iota(jnp.int32, (CHUNK, CHUNK), 1)
    causal = row >= col
    ones = causal.astype(bf16)

    def lanes(first, last):
        return slice(first * GROUP, last * GROUP)

    def span(t):
        return slice(t * ROWS, (t + 1) * ROWS)

    def prepare(t):
        gain = gainv[...].astype(bf16)
        for r in range(t * ROWS, (t + 1) * ROWS, STRIP):
            raw = tok[r : r + STRIP, :]
            feats = raw.shape[1]
            tok[r : r + STRIP, :] = raw * gain
            squares = raw * raw
            squares = squares[:, : feats // 2] + squares[:, feats // 2 :]
            squares = squares[:, : feats // 4] + squares[:, feats // 4 :]
            mean = jnp.sum(squares.astype(f32), axis=1, keepdims=True) * (1.0 / feats)
            scl[r : r + STRIP, :] = jnp.broadcast_to(lax.rsqrt(mean + norm_eps), (STRIP, GROUP))

    def project_states(t):
        here = span(t)
        both = dot(tok[here, :], w[:, lanes(0, 2)])
        scale = scl[here, :]
        xs[here, :] = (both[:, :GROUP] * scale).astype(bf16)
        val[here, :] = (both[:, GROUP:] * scale).astype(bf16)

    def logs(t):
        here = span(t)
        key = (1.0 - floorv[...]) * jax.nn.sigmoid(-xs[here, :].astype(f32))
        keyv[here, :] = key
        hi, low = split(jnp.log(1.0 - key) + leakv[here, :])
        terms[here, :GROUP] = hi
        terms[here, GROUP:] = low

    def piece(chunk):
        return slice(chunk * CHUNK, (chunk + 1) * CHUNK)

    def sums(chunk):
        both = dot(ones, terms[piece(chunk), :])
        emid[piece(chunk), :] = both[:, :GROUP] + both[:, GROUP:]

    def decays(chunk):
        at = piece(chunk)
        cum = emid[at, :]
        mid = cum[CHUNK // 2 - 1 : CHUNK // 2]
        last = cum[CHUNK - 1 : CHUNK]
        stats[chunk, 0:1] = mid
        stats[chunk, 2:3] = last
        emid[at, :] = jnp.exp(cum - mid)
        k_mid = keyv[at, :] * jnp.exp(mid - cum)
        kmid[at, :] = k_mid.astype(bf16)
        kend[at, :] = (k_mid * jnp.exp(last - mid)).astype(bf16)

    def own_state():
        state, offset = jnp.zeros((GROUP, GROUP), f32), jnp.zeros((1, GROUP), f32)
        for chunk in range(nchunk):
            at, last = piece(chunk), stats[chunk, 2:3]
            old[chunk] = state.astype(bf16)
            stats[chunk, 1:2] = offset
            state = state * jnp.exp(last) + dot(val[at, :], kend[at, :], ((0,), (0,)))
            offset = offset + last
        return state, offset

    def gated_inputs(both, factor):
        left = (both[:, :GROUP] * factor).astype(bf16).astype(f32)
        right = (both[:, GROUP:] * factor).astype(bf16).astype(f32)
        return (left * right).astype(bf16).astype(f32)

    with scope("load0"):
        smalls[0].wait()
        tok_copy(0).wait()
    for i in range(2, 7):
        w_copy(i).start()
    for copy in smalls[3:]:
        copy.start()
    with scope("prep0"):
        prepare(0)
    with scope("load1"):
        w_wait(0, 2)
        smalls[1].wait()
    for t in range(1, nb):
        with scope("tokwait"):
            tok_copy(t).wait()
        with scope("A"):
            prepare(t)
            project_states(t - 1)
        if t == 2:
            meet()

    def pack(slot, matrix, logs):
        hi = logs.astype(bf16)
        mid, low = split(logs - hi.astype(f32))
        slot[0:GROUP, :] = matrix.astype(bf16)
        r = lax.broadcasted_iota(jnp.int32, (LOGS, GROUP), 0)
        rows = jnp.where(r == 0, hi.astype(f32), jnp.where(r == 1, mid.astype(f32), low.astype(f32)))
        slot[GROUP : GROUP + LOGS, :] = rows.astype(bf16)

    def unpack(slot):
        logs = slot[GROUP : GROUP + LOGS, :].astype(f32)
        return slot[0:GROUP, :].astype(f32), logs[0:1] + logs[1:2] + logs[2:3]

    pad[0:HALO, :] = jnp.zeros((HALO, GROUP), f32)

    def convolve(first, size, conv_in, proj_b):
        taps_f = tapsv[...].astype(f32)
        total = taps_f[TAPS - 1 : TAPS] * conv_in
        for j in range(TAPS - 1):
            start = HALO - (TAPS - 1) + j + first
            total += taps_f[j : j + 1] * pad[start : start + size, :]
        return (rms(proj_b * total) * ggainv[...]).astype(bf16)

    def project_inputs(t):
        here = span(t)
        pad[HALO + t * ROWS : HALO + (t + 1) * ROWS, :] = gated_inputs(
            dot(tok[here, :], w[:, lanes(2, 4)]), scl[here, :]
        )

    def project_gates(t):
        here = span(t)
        both = dot(tok[here, :], w[:, lanes(4, 6)])
        factor = scl[here, :]
        prods[here, :] = (both[:, :GROUP] * factor).astype(bf16)
        gate[here, :] = (both[:, GROUP:] * factor).astype(bf16)

    def project_query(t):
        here = span(t)
        wide[here, :] = (dot(tok[here, :], w[:, lanes(6, 7)]) * scl[here, :]).astype(bf16)

    def send(kind, t):
        block_copy(kind, t, me, ahead, near_recv).start()
        block_copy(kind, t, me, behind, near_recv).start()
        block_copy(kind, t, me, partner, pair_recv).start()

    def conv(t):
        conv_in = pad[HALO + t * ROWS : HALO + (t + 1) * ROWS, :]
        put(1, t, convolve(t * ROWS, ROWS, conv_in, prods[span(t), :].astype(f32)))

    def reads(chunk):
        at = slice(chunk * CHUNK, (chunk + 1) * CHUNK)
        query = jax.nn.silu(wide[at, :].astype(f32))
        mid, before = stats[chunk, 0:1], stats[chunk, 1:2]
        q_mid = query * emid[at, :]
        q_all = q_mid * jnp.exp(mid)
        qdev[at, :] = (q_all * jnp.exp(before)).astype(bf16)
        scores = dot(q_mid.astype(bf16), kmid[at, :], ((1,), (1,)))
        scores = jnp.where(causal, scores, 0.0).astype(bf16)
        read[at, :] = dot(scores, val[at, :]) + dot(q_all.astype(bf16), old[chunk], ((1,), (1,)))

    def combine():
        with scope("ywait"):
            y_all.wait_recv()
        whole, logs = unpack(ybuf.at[0])
        for j in range(1, ny):
            more, log = unpack(ybuf.at[j])
            whole = whole * jnp.exp(log) + more
            logs = logs + log
        pack(zbuf.at[zz], whole, logs)
        with scope("readyz"):
            @pl.when(zz < nz - 1)
            def _():
                pl.semaphore_wait(ready_z.at[0], nz - 1 - zz)

        def send_z(target, _):
            z_copy(target).start()
            return 0

        lax.fori_loop(zz + 1, nz, send_z, 0)

    def first_rows():
        with scope("rimwait"):
            @pl.when(place > 0)
            def _():
                rim_arrival.wait_recv()
                pad[0:HALO, :] = rim[...]

        conv(0)
        send(1, 0)

    def share():
        with scope("colxwait"):
            far_cols_in.wait_recv()
        share_all(yy, y_ahead, 0)
        share_all(yy, y_behind, 1)

    def share_on():
        with scope("colywait"):
            shared_in(0).wait_recv()
        share_all(y_behind, y_ahead, 2)

    with scope("w23wait"):
        w_wait(2, 4)
        smalls[2].wait()
    with scope("A2"):
        project_states(nb - 1)
        logs(0)
        logs(1)
        project_inputs(nb - 1)
        logs(2)
        logs(3)
        tail[...] = pad[count : count + HALO, :]
        project_inputs(0)
        for chunk in range(nchunk):
            sums(chunk)
        for chunk in range(nchunk):
            decays(chunk)
        project_inputs(1)
        pack(ybuf.at[yy], *own_state())
    with scope("rimsend"):
        @pl.when(jnp.logical_and(yy == ny - 1, zz < nz - 1))
        def _():
            pl.semaphore_wait(ready_rim.at[0], 1)

        @pl.when(place < sp - 1)
        def _():
            rim_copy.start()

        for r in range(1, ny):
            y_copy(r).start()

    with scope("w46wait"):
        w_wait(4, 6)
        w_wait(6, 7)
        for copy in smalls[3:]:
            copy.wait()
    with scope("B1"):
        project_gates(1)
        conv(1)
        project_gates(0)
        send(1, 1)
    with scope("B2"):
        project_inputs(2)
        project_gates(2)
        conv(2)
        project_query(0)
        send(1, 2)
    first_rows()
    with scope("B3"):
        project_gates(3)
        conv(3)
        reads(0)
        reads(1)
        send(1, 3)
    combine()
    with scope("C2"):
        project_query(1)
        project_query(2)
        reads(2)
        reads(3)
        project_query(3)
        reads(4)
        reads(5)
    with scope("C3"):
        reads(6)
        reads(7)
    share()

    conv_order = [1, 2, 0, 3]
    with scope("relayconv"):
        for t in conv_order[:-1]:
            relay_first(1, t)

    incoming[...] = jnp.zeros_like(incoming)

    def hop_z(source, _):
        z_arrival(source).wait_recv()
        matrix, log = unpack(zbuf.at[source])
        incoming[...] = incoming[...] * jnp.exp(log) + matrix
        return 0

    with scope("hopz"):
        lax.fori_loop(0, zz, hop_z, 0)

    def hop_y(source, _):
        matrix, log = unpack(ybuf.at[source])
        incoming[...] = incoming[...] * jnp.exp(log) + matrix
        return 0

    lax.fori_loop(0, yy, hop_y, 0)

    def merge(t):
        here = span(t)
        total = read[here, :] + dot(qdev[here, :], incoming[...].astype(bf16), ((1,), (1,)))
        out = rms(total) * sgainv[...] * jax.nn.silu(gate[here, :].astype(f32))
        put(0, t, out.astype(bf16))
        send(0, t)

    with scope("merge"):
        for t in range(nb):
            merge(t)

    def conv_dot(t):
        with scope("convdot"):
            pair_wait(1, t)
            side = cols[tp : 2 * tp].reshape(tp * GROUP, ncols)
            acc[span(t), :] = dot(mixed[t, :, tp * GROUP :], side)

    with scope("relayconvlast"):
        relay_first(1, conv_order[-1])
    share_on()
    for t in range(nb - 1):
        with scope("relaystate"):
            relay_first(0, t)
        with scope("relayconv2"):
            relay_second(1, conv_order[t])
    with scope("colwait"):
        own_cols_done.wait()
        partner_cols_in.wait_recv()
        shared_in(1).wait_recv()
        shared_in(2).wait_recv()
    for t in conv_order[:-1]:
        conv_dot(t)
    with scope("relaystate"):
        relay_first(0, nb - 1)
    with scope("relayconv2last"):
        relay_second(1, conv_order[-1])

    def finish(t):
        with scope("finwait"):
            pair_wait(0, t)
        with scope("findot"):
            total = acc[span(t), :] + dot(mixed[t, :, : tp * GROUP], cols[0:tp].reshape(tp * GROUP, ncols))
            result[span(t), :] = total.astype(bf16)

    for t in range(nb):
        with scope("finfar"):
            relay_second(0, t)
        if t == 0:
            conv_dot(conv_order[-1])
        else:
            finish(t - 1)
    finish(nb - 1)

    with scope("drain"):
        blocks_sent.wait_send()
        colx_sent.wait_send()
        shares_sent.wait_send()
        y_all.wait_send()

        def drain_z(target, _):
            z_copy(target).wait_send()
            return 0

        lax.fori_loop(zz + 1, nz, drain_z, 0)

        @pl.when(place < sp - 1)
        def _():
            rim_copy.wait_send()


def body(
    tokens, in_gain, w_query, w_forget, w_input, w_outgate, w_conv_h, w_conv_b, w_conv_c,
    forget_floor, forget_leak, state_gain, conv_taps, group_gain, out_state, out_conv,
):
    count, feats = tokens.shape
    tp, sp = lax.axis_size("tp"), lax.axis_size("sp")
    ny, nz = NY, sp // NY
    ncols, nb = out_state.shape[1] // tp, count // ROWS
    nchunk = count // CHUNK
    hbm, vmem = pl.BlockSpec(memory_space=pltpu.HBM), pl.BlockSpec(memory_space=pltpu.VMEM)
    sems = pltpu.SemaphoreType.DMA
    return pl.pallas_call(
        functools.partial(fused_kernel, tp, ny, nz),
        in_specs=[hbm] * 16,
        out_specs=vmem,
        out_shape=jax.ShapeDtypeStruct((count, ncols), bf16),
        scratch_shapes=[
            pltpu.VMEM((count, feats), bf16),
            pltpu.VMEM((feats, 7 * GROUP), bf16),
            pltpu.VMEM((count, GROUP), f32),
            pltpu.VMEM((2 * tp, GROUP, ncols), bf16),
            pltpu.VMEM((nb, ROWS, 2 * tp * GROUP), bf16),
            pltpu.VMEM((count, GROUP), bf16),
            pltpu.VMEM((count, GROUP), bf16),
            pltpu.VMEM((count, GROUP), bf16),
            pltpu.VMEM((count, GROUP), f32),
            pltpu.VMEM((nchunk, GROUP, GROUP), bf16),
            pltpu.VMEM((nchunk, HALO, GROUP), f32),
            pltpu.VMEM((count, GROUP), bf16),
            pltpu.VMEM((count, GROUP), f32),
            pltpu.VMEM((count, GROUP), bf16),
            pltpu.VMEM((count, GROUP), f32),
            pltpu.VMEM((count, ncols), f32),
            pltpu.VMEM((1, feats), f32),
            pltpu.VMEM((1, GROUP), f32),
            pltpu.VMEM((1, GROUP), f32),
            pltpu.VMEM((1, GROUP), f32),
            pltpu.VMEM((TAPS, GROUP), bf16),
            pltpu.VMEM((count, GROUP), bf16),
            pltpu.VMEM((count, GROUP), bf16),
            pltpu.VMEM((count, GROUP), f32),
            pltpu.VMEM((count, 2 * GROUP), bf16),
            pltpu.VMEM((count, GROUP), bf16),
            pltpu.VMEM((HALO + count, GROUP), f32),
            pltpu.VMEM((GROUP, GROUP), f32),
            pltpu.VMEM((ny, GROUP + LOGS, GROUP), bf16),
            pltpu.VMEM((nz, GROUP + LOGS, GROUP), bf16),
            pltpu.VMEM((HALO, GROUP), f32),
            pltpu.VMEM((HALO, GROUP), f32),
            sems((nb,)), sems((4,)), sems((6,)), sems((1,)),
            pltpu.SemaphoreType.REGULAR((1,)), pltpu.SemaphoreType.REGULAR((1,)),
            sems((1,)), sems((2,)), sems((1,)), sems((3,)),
            sems((1,)), sems((1,)), sems((nz,)), sems((nz,)), sems((1,)), sems((1,)),
            sems((1,)), sems((2, nb)), sems((2, nb)), sems((2, nb)),
        ],
        compiler_params=pltpu.CompilerParams(
            vmem_limit_bytes=40 * 2**20, collective_id=0, has_side_effects=True
        ),
    )(*[pltpu.with_memory_space_constraint(a, pltpu.HBM) for a in (
        tokens, in_gain[None], w_query, w_forget, w_input, w_outgate, w_conv_h, w_conv_b, w_conv_c,
        forget_floor[None], forget_leak, state_gain[None], conv_taps, group_gain[None],
        out_state, out_conv,
    )])


def solution(mesh):
    cols, rows = P(None, "tp"), P("tp", None)
    in_specs = (
        P("sp", None), P(), cols, cols, cols, cols, cols, cols, cols,
        P("tp"), P("sp", "tp"), P(), cols, P(), rows, rows,
    )
    return jax.shard_map(
        body, mesh=mesh, in_specs=in_specs, out_specs=P("sp", "tp"), check_vma=False
    )
```

```python
import functools

import jax
import jax.numpy as jnp
from jax import lax
from jax.experimental import pallas as pl
from jax.experimental.pallas import tpu as pltpu
from jax.sharding import PartitionSpec as P

GROUP = 128
CHUNK = 128
ROWS = 256
TAPS = 3
HALO = 8
NY = 4
LOGS = 16
STRIP = 16

norm_eps = 1e-06
f32 = jnp.float32
bf16 = jnp.bfloat16


scope = jax.named_scope


def dot(a, b, dims=((1,), (0,))):
    return lax.dot_general(a, b, (dims, ((), ())), preferred_element_type=f32)


def rms(values):
    return values * lax.rsqrt(jnp.mean(values * values, axis=-1, keepdims=True) + norm_eps)


def split(values):
    hi = values.astype(bf16)
    return hi, (values - hi.astype(f32)).astype(bf16)


def fused_kernel(
    tp, ny, nz,
    tokens, in_gain, wq, wf, wi, wg, wh, wb, wc, floor, leak, state_gain, taps, group_gain,
    out_state, out_conv, result,
    tok, w, leakv, cols, mixed, xs, kmid, val, emid, old, stats, gate, read, qdev, scl, acc,
    gainv, floorv, sgainv, ggainv, tapsv, prods, wide, keyv, terms, kend,
    pad, incoming, ybuf, zbuf, rim, tail,
    tok_sem, w_sem, small_sem, own_sem, ready_z, ready_rim,
    colx_send, colx_recv, coly_send, coly_recv,
    y_send, y_recv, z_send, z_recv, rim_send, rim_recv, blk_send, near_recv, far_recv, pair_recv,
):
    me, place = lax.axis_index("tp"), lax.axis_index("sp")
    sp = ny * nz
    core, chip = lax.rem(me, 2), lax.div(me, 2)
    partner = me + 1 - 2 * core
    yy, zz = lax.rem(place, ny), lax.div(place, ny)
    far = lax.rem(me + 4, tp)
    ahead = lax.rem(me + tp + 2 - 4 * core, tp)
    behind = lax.rem(me + tp - 2 + 4 * core, tp)
    y_ahead = lax.rem(yy + ny + 1 - 2 * core, ny)
    y_behind = lax.rem(yy + ny - 1 + 2 * core, ny)
    count, ncols = result.shape
    nb = count // ROWS
    nchunk = count // CHUNK
    part = GROUP // ny
    per = ROWS // CHUNK
    outs = (out_state, out_conv)

    def rows_at(t):
        return pl.ds(pl.multiple_of(t * ROWS, ROWS), ROWS)

    def tok_copy(t):
        return pltpu.make_async_copy(tokens.at[rows_at(t)], tok.at[rows_at(t)], tok_sem.at[t])

    weights = (wf, wi, wc, wh, wb, wg, wq)

    def w_copy(i):
        return pltpu.make_async_copy(
            weights[i], w.at[:, i * GROUP : (i + 1) * GROUP], w_sem.at[i // 2]
        )

    def w_wait(first, last):
        ref = w.at[:, first * GROUP : last * GROUP]
        pltpu.make_async_copy(ref, ref, w_sem.at[first // 2]).wait()

    smalls = (
        pltpu.make_async_copy(in_gain, gainv, small_sem.at[0]),
        pltpu.make_async_copy(floor, floorv, small_sem.at[1]),
        pltpu.make_async_copy(leak, leakv, small_sem.at[2]),
        pltpu.make_async_copy(taps, tapsv, small_sem.at[3]),
        pltpu.make_async_copy(group_gain, ggainv, small_sem.at[4]),
        pltpu.make_async_copy(state_gain, sgainv, small_sem.at[5]),
    )

    def col_slice(target):
        return pl.ds(pl.multiple_of(target * ncols, ncols), ncols)

    mine_rows = pl.ds(pl.multiple_of(yy * part, part), part)

    def landed(ref, send, recv):
        return pltpu.make_async_remote_copy(ref, ref, send, recv, device_id={"tp": partner})

    def own_cols(kind):
        return pltpu.make_async_copy(
            outs[kind].at[:, col_slice(me)], cols.at[kind * tp + me], own_sem.at[0]
        )

    own_cols_done = pltpu.make_async_copy(
        cols.at[pl.ds(0, 2)], cols.at[pl.ds(0, 2)], own_sem.at[0]
    )

    def partner_cols(kind):
        return pltpu.make_async_remote_copy(
            outs[kind].at[:, col_slice(partner)], cols.at[kind * tp + me],
            colx_send.at[0], colx_recv.at[1], device_id={"tp": partner},
        )

    def far_cols(kind, k):
        target = lax.rem(2 * chip + 2 + k, tp)
        return pltpu.make_async_remote_copy(
            outs[kind].at[mine_rows, col_slice(target)], cols.at[kind * tp + me, mine_rows],
            colx_send.at[0], colx_recv.at[0], device_id={"tp": target},
        )

    far_units = 2 * (tp - 2) // ny
    far_cols_in = landed(cols.at[pl.ds(0, far_units)], colx_send.at[0], colx_recv.at[0])
    partner_cols_in = landed(cols.at[pl.ds(0, 2)], colx_send.at[0], colx_recv.at[1])
    colx_sent = landed(cols.at[pl.ds(0, far_units + 2)], colx_send.at[0], colx_recv.at[0])

    def share_cols(kind, j, origin, target, slot):
        pair = pl.ds(kind * tp + lax.rem(2 * chip + 2 * j, tp), 2)
        ref = cols.at[pair, pl.ds(pl.multiple_of(origin * part, part), part)]
        return pltpu.make_async_remote_copy(
            ref, ref, coly_send.at[0], coly_recv.at[slot], device_id={"sp": zz * ny + target}
        )

    def share_all(origin, target, slot):
        for kind in range(2):
            for j in range(1, tp // 2):
                share_cols(kind, j, origin, target, slot).start()

    def shared_in(slot):
        return landed(cols.at[pl.ds(0, far_units)], coly_send.at[0], coly_recv.at[slot])

    shares_sent = landed(cols.at[pl.ds(0, 3 * far_units)], coly_send.at[0], coly_recv.at[0])

    def y_copy(r):
        ref = ybuf.at[yy]
        return pltpu.make_async_remote_copy(
            ref, ref, y_send.at[0], y_recv.at[0],
            device_id={"sp": zz * ny + lax.rem(yy + r, ny)},
        )

    y_all = landed(ybuf.at[pl.ds(0, ny - 1)], y_send.at[0], y_recv.at[0])

    def z_copy(target):
        ref = zbuf.at[zz]
        return pltpu.make_async_remote_copy(
            ref, ref, z_send.at[target], z_recv.at[zz], device_id={"sp": target * ny + yy}
        )

    def z_arrival(source):
        ref = zbuf.at[source]
        return pltpu.make_async_remote_copy(
            ref, ref, z_send.at[source], z_recv.at[source], device_id={"sp": source * ny + yy}
        )

    rim_copy = pltpu.make_async_remote_copy(
        tail, rim, rim_send.at[0], rim_recv.at[0], device_id={"sp": place + 1}
    )
    rim_arrival = pltpu.make_async_remote_copy(
        tail, rim, rim_send.at[0], rim_recv.at[0], device_id={"sp": place - 1}
    )

    def block_copy(kind, t, origin, target, recv):
        lanes = pl.ds(pl.multiple_of((kind * tp + origin) * GROUP, GROUP), GROUP)
        ref = mixed.at[t, :, lanes]
        return pltpu.make_async_remote_copy(
            ref, ref, blk_send.at[0], recv.at[kind, t], device_id={"tp": target}
        )

    def relay_first(kind, t):
        landed(mixed.at[t, :, 0 : 2 * GROUP], blk_send.at[0], near_recv.at[kind, t]).wait_recv()
        block_copy(kind, t, behind, ahead, far_recv).start()
        block_copy(kind, t, behind, partner, pair_recv).start()
        block_copy(kind, t, ahead, partner, pair_recv).start()

    def relay_second(kind, t):
        landed(mixed.at[t, :, 0:GROUP], blk_send.at[0], far_recv.at[kind, t]).wait_recv()
        block_copy(kind, t, far, partner, pair_recv).start()

    def pair_wait(kind, t):
        half = mixed.at[t, :, 0 : tp // 2 * GROUP]
        landed(half, blk_send.at[0], pair_recv.at[kind, t]).wait_recv()

    blocks_sent = landed(
        mixed.at[:, :, 0 : 2 * (tp - 1) * GROUP], blk_send.at[0], pair_recv.at[0, 0]
    )

    def put(kind, t, value):
        lanes = pl.ds(pl.multiple_of((kind * tp + me) * GROUP, GROUP), GROUP)
        mixed[t, :, lanes] = value

    smalls[0].start()
    tok_copy(0).start()
    w_copy(0).start()
    w_copy(1).start()
    smalls[1].start()
    barrier = pltpu.get_barrier_semaphore()
    for k in range(1, tp):
        pl.semaphore_signal(barrier, inc=1, device_id={"tp": lax.rem(me + k, tp)})
    for r in range(1, ny):
        pl.semaphore_signal(barrier, inc=1, device_id={"sp": zz * ny + lax.rem(yy + r, ny)})

    def greet_z(target, _):
        pl.semaphore_signal(barrier, inc=1, device_id={"sp": target * ny + yy})
        return 0

    lax.fori_loop(zz + 1, nz, greet_z, 0)

    @pl.when(jnp.logical_and(yy == ny - 1, zz < nz - 1))
    def _():
        pl.semaphore_signal(barrier, inc=1, device_id={"sp": place + 1})

    for t in range(1, nb):
        tok_copy(t).start()
    smalls[2].start()

    def meet():
        with scope("barrier"):
            across = jnp.where(yy == 0, jnp.minimum(zz, 1), 0)
            pl.semaphore_wait(barrier, tp + ny - 2 + zz + across)

        def ready(target, _):
            pl.semaphore_signal(ready_z.at[0], inc=1, device_id={"sp": target * ny + yy})
            return 0

        lax.fori_loop(0, zz, ready, 0)

        @pl.when(jnp.logical_and(yy == 0, zz > 0))
        def _():
            pl.semaphore_signal(ready_rim.at[0], inc=1, device_id={"sp": place - 1})

        for kind in range(2):
            for k in range(tp - 2):
                far_cols(kind, k).start()
        for kind in range(2):
            partner_cols(kind).start()
            own_cols(kind).start()

    row = lax.broadcasted_iota(jnp.int32, (CHUNK, CHUNK), 0)
    col = lax.broadcasted_iota(jnp.int32, (CHUNK, CHUNK), 1)
    causal = row >= col
    ones = causal.astype(bf16)

    def lanes(first, last):
        return slice(first * GROUP, last * GROUP)

    def span(t):
        return slice(t * ROWS, (t + 1) * ROWS)

    def prepare(t):
        gain = gainv[...].astype(bf16)
        for r in range(t * ROWS, (t + 1) * ROWS, STRIP):
            raw = tok[r : r + STRIP, :]
            feats = raw.shape[1]
            tok[r : r + STRIP, :] = raw * gain
            squares = raw * raw
            squares = squares[:, : feats // 2] + squares[:, feats // 2 :]
            squares = squares[:, : feats // 4] + squares[:, feats // 4 :]
            mean = jnp.sum(squares.astype(f32), axis=1, keepdims=True) * (1.0 / feats)
            scl[r : r + STRIP, :] = jnp.broadcast_to(lax.rsqrt(mean + norm_eps), (STRIP, GROUP))

    def project_states(t):
        here = span(t)
        both = dot(tok[here, :], w[:, lanes(0, 2)])
        scale = scl[here, :]
        xs[here, :] = (both[:, :GROUP] * scale).astype(bf16)
        val[here, :] = (both[:, GROUP:] * scale).astype(bf16)

    def logs(t):
        here = span(t)
        key = (1.0 - floorv[...]) * jax.nn.sigmoid(-xs[here, :].astype(f32))
        keyv[here, :] = key
        hi, low = split(jnp.log(1.0 - key) + leakv[here, :])
        terms[here, :GROUP] = hi
        terms[here, GROUP:] = low

    def piece(chunk):
        return slice(chunk * CHUNK, (chunk + 1) * CHUNK)

    def sums(chunk):
        both = dot(ones, terms[piece(chunk), :])
        emid[piece(chunk), :] = both[:, :GROUP] + both[:, GROUP:]

    def decays(chunk):
        at = piece(chunk)
        cum = emid[at, :]
        mid = cum[CHUNK // 2 - 1 : CHUNK // 2]
        last = cum[CHUNK - 1 : CHUNK]
        stats[chunk, 0:1] = mid
        stats[chunk, 2:3] = last
        emid[at, :] = jnp.exp(cum - mid)
        k_mid = keyv[at, :] * jnp.exp(mid - cum)
        kmid[at, :] = k_mid.astype(bf16)
        kend[at, :] = (k_mid * jnp.exp(last - mid)).astype(bf16)

    def own_state():
        state, offset = jnp.zeros((GROUP, GROUP), f32), jnp.zeros((1, GROUP), f32)
        for chunk in range(nchunk):
            at, last = piece(chunk), stats[chunk, 2:3]
            old[chunk] = state.astype(bf16)
            stats[chunk, 1:2] = offset
            state = state * jnp.exp(last) + dot(val[at, :], kend[at, :], ((0,), (0,)))
            offset = offset + last
        return state, offset

    def gated_inputs(both, factor):
        left = (both[:, :GROUP] * factor).astype(bf16).astype(f32)
        right = (both[:, GROUP:] * factor).astype(bf16).astype(f32)
        return (left * right).astype(bf16).astype(f32)

    with scope("load0"):
        smalls[0].wait()
        tok_copy(0).wait()
    for i in range(2, 7):
        w_copy(i).start()
    for copy in smalls[3:]:
        copy.start()
    with scope("prep0"):
        prepare(0)
    with scope("load1"):
        w_wait(0, 2)
        smalls[1].wait()
    for t in range(1, nb):
        with scope("tokwait"):
            tok_copy(t).wait()
        with scope("A"):
            project_states(t - 1)
            prepare(t)
        if t == 2:
            meet()

    def pack(slot, matrix, logs):
        hi = logs.astype(bf16)
        mid, low = split(logs - hi.astype(f32))
        slot[0:GROUP, :] = matrix.astype(bf16)
        r = lax.broadcasted_iota(jnp.int32, (LOGS, GROUP), 0)
        rows = jnp.where(r == 0, hi.astype(f32), jnp.where(r == 1, mid.astype(f32), low.astype(f32)))
        slot[GROUP : GROUP + LOGS, :] = rows.astype(bf16)

    def unpack(slot):
        logs = slot[GROUP : GROUP + LOGS, :].astype(f32)
        return slot[0:GROUP, :].astype(f32), logs[0:1] + logs[1:2] + logs[2:3]

    pad[0:HALO, :] = jnp.zeros((HALO, GROUP), f32)

    def convolve(first, size, conv_in, proj_b):
        taps_f = tapsv[...].astype(f32)
        total = taps_f[TAPS - 1 : TAPS] * conv_in
        for j in range(TAPS - 1):
            start = HALO - (TAPS - 1) + j + first
            total += taps_f[j : j + 1] * pad[start : start + size, :]
        return (rms(proj_b * total) * ggainv[...]).astype(bf16)

    def project_inputs(t):
        here = span(t)
        pad[HALO + t * ROWS : HALO + (t + 1) * ROWS, :] = gated_inputs(
            dot(tok[here, :], w[:, lanes(2, 4)]), scl[here, :]
        )

    def project_gates(t):
        here = span(t)
        both = dot(tok[here, :], w[:, lanes(4, 6)])
        factor = scl[here, :]
        prods[here, :] = (both[:, :GROUP] * factor).astype(bf16)
        gate[here, :] = (both[:, GROUP:] * factor).astype(bf16)

    def project_query(t):
        here = span(t)
        wide[here, :] = (dot(tok[here, :], w[:, lanes(6, 7)]) * scl[here, :]).astype(bf16)

    def send(kind, t):
        block_copy(kind, t, me, ahead, near_recv).start()
        block_copy(kind, t, me, behind, near_recv).start()
        block_copy(kind, t, me, partner, pair_recv).start()

    def conv(t):
        conv_in = pad[HALO + t * ROWS : HALO + (t + 1) * ROWS, :]
        put(1, t, convolve(t * ROWS, ROWS, conv_in, prods[span(t), :].astype(f32)))

    def reads(chunk):
        at = slice(chunk * CHUNK, (chunk + 1) * CHUNK)
        query = jax.nn.silu(wide[at, :].astype(f32))
        mid, before = stats[chunk, 0:1], stats[chunk, 1:2]
        q_mid = query * emid[at, :]
        q_all = q_mid * jnp.exp(mid)
        qdev[at, :] = (q_all * jnp.exp(before)).astype(bf16)
        scores = dot(q_mid.astype(bf16), kmid[at, :], ((1,), (1,)))
        scores = jnp.where(causal, scores, 0.0).astype(bf16)
        read[at, :] = dot(scores, val[at, :]) + dot(q_all.astype(bf16), old[chunk], ((1,), (1,)))

    def combine():
        with scope("ywait"):
            y_all.wait_recv()
        whole, logs = unpack(ybuf.at[0])
        for j in range(1, ny):
            more, log = unpack(ybuf.at[j])
            whole = whole * jnp.exp(log) + more
            logs = logs + log
        pack(zbuf.at[zz], whole, logs)
        with scope("readyz"):
            @pl.when(zz < nz - 1)
            def _():
                pl.semaphore_wait(ready_z.at[0], nz - 1 - zz)

        def send_z(step, _):
            z_copy(nz - 1 - step).start()
            return 0

        lax.fori_loop(0, nz - 1 - zz, send_z, 0)

    def first_rows():
        with scope("rimwait"):
            @pl.when(place > 0)
            def _():
                rim_arrival.wait_recv()
                pad[0:HALO, :] = rim[...]

        conv(0)
        send(1, 0)

    def share():
        with scope("colxwait"):
            far_cols_in.wait_recv()
        share_all(yy, y_ahead, 0)
        share_all(yy, y_behind, 1)

    def share_on():
        with scope("colywait"):
            shared_in(0).wait_recv()
        share_all(y_behind, y_ahead, 2)

    with scope("w23wait"):
        w_wait(2, 4)
        smalls[2].wait()
    with scope("A2"):
        project_states(nb - 1)
        logs(0)
        logs(1)
        project_inputs(nb - 1)
        logs(2)
        logs(3)
        tail[...] = pad[count : count + HALO, :]
        project_inputs(0)
        for chunk in range(nchunk):
            sums(chunk)
        for chunk in range(nchunk):
            decays(chunk)
        project_inputs(1)
        pack(ybuf.at[yy], *own_state())
    with scope("rimsend"):
        @pl.when(jnp.logical_and(yy == ny - 1, zz < nz - 1))
        def _():
            pl.semaphore_wait(ready_rim.at[0], 1)

        @pl.when(place < sp - 1)
        def _():
            rim_copy.start()

        for r in range(1, ny):
            y_copy(r).start()

    with scope("w46wait"):
        w_wait(4, 6)
        w_wait(6, 7)
        for copy in smalls[3:]:
            copy.wait()
    with scope("B1"):
        project_gates(1)
        conv(1)
        project_gates(0)
        send(1, 1)
    with scope("B2"):
        project_inputs(2)
        project_gates(2)
        conv(2)
        project_query(0)
        send(1, 2)
    first_rows()
    with scope("B3"):
        project_gates(3)
        conv(3)
        reads(0)
        reads(1)
        send(1, 3)
    combine()
    share()
    with scope("C2"):
        project_query(1)
        project_query(2)
        reads(2)
        reads(3)
        project_query(3)
        reads(4)
        reads(5)
    with scope("C3"):
        reads(6)
        reads(7)

    conv_order = [1, 2, 0, 3]
    with scope("relayconv"):
        for t in conv_order:
            relay_first(1, t)

    incoming[...] = jnp.zeros_like(incoming)

    def hop_z(source, _):
        z_arrival(source).wait_recv()
        matrix, log = unpack(zbuf.at[source])
        incoming[...] = incoming[...] * jnp.exp(log) + matrix
        return 0

    with scope("hopz"):
        lax.fori_loop(0, zz, hop_z, 0)

    def hop_y(source, _):
        matrix, log = unpack(ybuf.at[source])
        incoming[...] = incoming[...] * jnp.exp(log) + matrix
        return 0

    lax.fori_loop(0, yy, hop_y, 0)

    def merge(t):
        here = span(t)
        total = read[here, :] + dot(qdev[here, :], incoming[...].astype(bf16), ((1,), (1,)))
        out = rms(total) * sgainv[...] * jax.nn.silu(gate[here, :].astype(f32))
        put(0, t, out.astype(bf16))
        send(0, t)

    with scope("merge"):
        for t in range(nb):
            merge(t)

    def conv_dot(t):
        with scope("convdot"):
            pair_wait(1, t)
            side = cols[tp : 2 * tp].reshape(tp * GROUP, ncols)
            acc[span(t), :] = dot(mixed[t, :, tp * GROUP :], side)

    share_on()
    with scope("relayconv2"):
        for t in conv_order[:-1]:
            relay_second(1, t)
    for t in range(nb):
        with scope("relaystate"):
            relay_first(0, t)
        if t == 1:
            with scope("colwait"):
                own_cols_done.wait()
                partner_cols_in.wait_recv()
                shared_in(1).wait_recv()
                shared_in(2).wait_recv()
        if t > 0:
            conv_dot(conv_order[t - 1])
    with scope("relayconv2last"):
        relay_second(1, conv_order[-1])

    def finish(t):
        with scope("finwait"):
            pair_wait(0, t)
        with scope("findot"):
            total = acc[span(t), :] + dot(mixed[t, :, : tp * GROUP], cols[0:tp].reshape(tp * GROUP, ncols))
            result[span(t), :] = total.astype(bf16)

    for t in range(nb):
        with scope("finfar"):
            relay_second(0, t)
        if t > 0:
            finish(t - 1)
    conv_dot(conv_order[-1])
    finish(nb - 1)

    with scope("drain"):
        blocks_sent.wait_send()
        colx_sent.wait_send()
        shares_sent.wait_send()
        y_all.wait_send()

        def drain_z(target, _):
            z_copy(target).wait_send()
            return 0

        lax.fori_loop(zz + 1, nz, drain_z, 0)

        @pl.when(place < sp - 1)
        def _():
            rim_copy.wait_send()


def body(
    tokens, in_gain, w_query, w_forget, w_input, w_outgate, w_conv_h, w_conv_b, w_conv_c,
    forget_floor, forget_leak, state_gain, conv_taps, group_gain, out_state, out_conv,
):
    count, feats = tokens.shape
    tp, sp = lax.axis_size("tp"), lax.axis_size("sp")
    ny, nz = NY, sp // NY
    ncols, nb = out_state.shape[1] // tp, count // ROWS
    nchunk = count // CHUNK
    hbm, vmem = pl.BlockSpec(memory_space=pltpu.HBM), pl.BlockSpec(memory_space=pltpu.VMEM)
    sems = pltpu.SemaphoreType.DMA
    return pl.pallas_call(
        functools.partial(fused_kernel, tp, ny, nz),
        in_specs=[hbm] * 16,
        out_specs=vmem,
        out_shape=jax.ShapeDtypeStruct((count, ncols), bf16),
        scratch_shapes=[
            pltpu.VMEM((count, feats), bf16),
            pltpu.VMEM((feats, 7 * GROUP), bf16),
            pltpu.VMEM((count, GROUP), f32),
            pltpu.VMEM((2 * tp, GROUP, ncols), bf16),
            pltpu.VMEM((nb, ROWS, 2 * tp * GROUP), bf16),
            pltpu.VMEM((count, GROUP), bf16),
            pltpu.VMEM((count, GROUP), bf16),
            pltpu.VMEM((count, GROUP), bf16),
            pltpu.VMEM((count, GROUP), f32),
            pltpu.VMEM((nchunk, GROUP, GROUP), bf16),
            pltpu.VMEM((nchunk, HALO, GROUP), f32),
            pltpu.VMEM((count, GROUP), bf16),
            pltpu.VMEM((count, GROUP), f32),
            pltpu.VMEM((count, GROUP), bf16),
            pltpu.VMEM((count, GROUP), f32),
            pltpu.VMEM((count, ncols), f32),
            pltpu.VMEM((1, feats), f32),
            pltpu.VMEM((1, GROUP), f32),
            pltpu.VMEM((1, GROUP), f32),
            pltpu.VMEM((1, GROUP), f32),
            pltpu.VMEM((TAPS, GROUP), bf16),
            pltpu.VMEM((count, GROUP), bf16),
            pltpu.VMEM((count, GROUP), bf16),
            pltpu.VMEM((count, GROUP), f32),
            pltpu.VMEM((count, 2 * GROUP), bf16),
            pltpu.VMEM((count, GROUP), bf16),
            pltpu.VMEM((HALO + count, GROUP), f32),
            pltpu.VMEM((GROUP, GROUP), f32),
            pltpu.VMEM((ny, GROUP + LOGS, GROUP), bf16),
            pltpu.VMEM((nz, GROUP + LOGS, GROUP), bf16),
            pltpu.VMEM((HALO, GROUP), f32),
            pltpu.VMEM((HALO, GROUP), f32),
            sems((nb,)), sems((4,)), sems((6,)), sems((1,)),
            pltpu.SemaphoreType.REGULAR((1,)), pltpu.SemaphoreType.REGULAR((1,)),
            sems((1,)), sems((2,)), sems((1,)), sems((3,)),
            sems((1,)), sems((1,)), sems((nz,)), sems((nz,)), sems((1,)), sems((1,)),
            sems((1,)), sems((2, nb)), sems((2, nb)), sems((2, nb)),
        ],
        compiler_params=pltpu.CompilerParams(
            vmem_limit_bytes=40 * 2**20, collective_id=0, has_side_effects=True
        ),
    )(*[pltpu.with_memory_space_constraint(a, pltpu.HBM) for a in (
        tokens, in_gain[None], w_query, w_forget, w_input, w_outgate, w_conv_h, w_conv_b, w_conv_c,
        forget_floor[None], forget_leak, state_gain[None], conv_taps, group_gain[None],
        out_state, out_conv,
    )])


def solution(mesh):
    cols, rows = P(None, "tp"), P("tp", None)
    in_specs = (
        P("sp", None), P(), cols, cols, cols, cols, cols, cols, cols,
        P("tp"), P("sp", "tp"), P(), cols, P(), rows, rows,
    )
    return jax.shard_map(
        body, mesh=mesh, in_specs=in_specs, out_specs=P("sp", "tp"), check_vma=False
    )
```

```python
import functools

import jax
import jax.numpy as jnp
from jax import lax
from jax.experimental import pallas as pl
from jax.experimental.pallas import tpu as pltpu
from jax.sharding import PartitionSpec as P

GROUP = 128
CHUNK = 128
ROWS = 256
TAPS = 3
HALO = 8
NY = 4
LOGS = 16
STRIP = 16

norm_eps = 1e-06
f32 = jnp.float32
bf16 = jnp.bfloat16


scope = jax.named_scope


def dot(a, b, dims=((1,), (0,))):
    return lax.dot_general(a, b, (dims, ((), ())), preferred_element_type=f32)


def rms(values):
    return values * lax.rsqrt(jnp.mean(values * values, axis=-1, keepdims=True) + norm_eps)


def split(values):
    hi = values.astype(bf16)
    return hi, (values - hi.astype(f32)).astype(bf16)


def fused_kernel(
    tp, ny, nz,
    tokens, in_gain, wq, wf, wi, wg, wh, wb, wc, floor, leak, state_gain, taps, group_gain,
    out_state, out_conv, result,
    tok, w, leakv, cols, mixed, xs, kmid, val, emid, old, stats, gate, read, qdev, scl, acc,
    gainv, floorv, sgainv, ggainv, tapsv, prods, wide, keyv, terms, kend,
    pad, incoming, ybuf, zbuf, rim, tail,
    tok_sem, w_sem, small_sem, own_sem, ready_z, ready_rim,
    colx_send, colx_recv, coly_send, coly_recv,
    y_send, y_recv, z_send, z_recv, rim_send, rim_recv, blk_send, near_recv, far_recv, pair_recv,
):
    me, place = lax.axis_index("tp"), lax.axis_index("sp")
    sp = ny * nz
    core, chip = lax.rem(me, 2), lax.div(me, 2)
    partner = me + 1 - 2 * core
    yy, zz = lax.rem(place, ny), lax.div(place, ny)
    far = lax.rem(me + 4, tp)
    ahead = lax.rem(me + tp + 2 - 4 * core, tp)
    behind = lax.rem(me + tp - 2 + 4 * core, tp)
    y_ahead = lax.rem(yy + ny + 1 - 2 * core, ny)
    y_behind = lax.rem(yy + ny - 1 + 2 * core, ny)
    count, ncols = result.shape
    nb = count // ROWS
    nchunk = count // CHUNK
    part = GROUP // ny
    per = ROWS // CHUNK
    outs = (out_state, out_conv)

    def rows_at(t):
        return pl.ds(pl.multiple_of(t * ROWS, ROWS), ROWS)

    def tok_copy(t):
        return pltpu.make_async_copy(tokens.at[rows_at(t)], tok.at[rows_at(t)], tok_sem.at[t])

    weights = (wf, wi, wc, wh, wb, wg, wq)

    def w_copy(i):
        return pltpu.make_async_copy(
            weights[i], w.at[:, i * GROUP : (i + 1) * GROUP], w_sem.at[i // 2]
        )

    def w_wait(first, last):
        ref = w.at[:, first * GROUP : last * GROUP]
        pltpu.make_async_copy(ref, ref, w_sem.at[first // 2]).wait()

    smalls = (
        pltpu.make_async_copy(in_gain, gainv, small_sem.at[0]),
        pltpu.make_async_copy(floor, floorv, small_sem.at[1]),
        pltpu.make_async_copy(leak, leakv, small_sem.at[2]),
        pltpu.make_async_copy(taps, tapsv, small_sem.at[3]),
        pltpu.make_async_copy(group_gain, ggainv, small_sem.at[4]),
        pltpu.make_async_copy(state_gain, sgainv, small_sem.at[5]),
    )

    def col_slice(target):
        return pl.ds(pl.multiple_of(target * ncols, ncols), ncols)

    mine_rows = pl.ds(pl.multiple_of(yy * part, part), part)

    def landed(ref, send, recv):
        return pltpu.make_async_remote_copy(ref, ref, send, recv, device_id={"tp": partner})

    def own_cols(kind):
        return pltpu.make_async_copy(
            outs[kind].at[:, col_slice(me)], cols.at[kind * tp + me], own_sem.at[0]
        )

    own_cols_done = pltpu.make_async_copy(
        cols.at[pl.ds(0, 2)], cols.at[pl.ds(0, 2)], own_sem.at[0]
    )

    def partner_cols(kind):
        return pltpu.make_async_remote_copy(
            outs[kind].at[:, col_slice(partner)], cols.at[kind * tp + me],
            colx_send.at[0], colx_recv.at[1], device_id={"tp": partner},
        )

    def far_cols(kind, k):
        target = lax.rem(2 * chip + 2 + k, tp)
        return pltpu.make_async_remote_copy(
            outs[kind].at[mine_rows, col_slice(target)], cols.at[kind * tp + me, mine_rows],
            colx_send.at[0], colx_recv.at[0], device_id={"tp": target},
        )

    far_units = 2 * (tp - 2) // ny
    far_cols_in = landed(cols.at[pl.ds(0, far_units)], colx_send.at[0], colx_recv.at[0])
    partner_cols_in = landed(cols.at[pl.ds(0, 2)], colx_send.at[0], colx_recv.at[1])
    colx_sent = landed(cols.at[pl.ds(0, far_units + 2)], colx_send.at[0], colx_recv.at[0])

    def share_cols(kind, j, origin, target, slot):
        pair = pl.ds(kind * tp + lax.rem(2 * chip + 2 * j, tp), 2)
        ref = cols.at[pair, pl.ds(pl.multiple_of(origin * part, part), part)]
        return pltpu.make_async_remote_copy(
            ref, ref, coly_send.at[0], coly_recv.at[slot], device_id={"sp": zz * ny + target}
        )

    def share_all(origin, target, slot):
        for kind in range(2):
            for j in range(1, tp // 2):
                share_cols(kind, j, origin, target, slot).start()

    def shared_in(slot):
        return landed(cols.at[pl.ds(0, far_units)], coly_send.at[0], coly_recv.at[slot])

    shares_sent = landed(cols.at[pl.ds(0, 3 * far_units)], coly_send.at[0], coly_recv.at[0])

    def y_copy(r):
        ref = ybuf.at[yy]
        return pltpu.make_async_remote_copy(
            ref, ref, y_send.at[0], y_recv.at[0],
            device_id={"sp": zz * ny + lax.rem(yy + r, ny)},
        )

    y_all = landed(ybuf.at[pl.ds(0, ny - 1)], y_send.at[0], y_recv.at[0])

    def z_copy(target):
        ref = zbuf.at[zz]
        return pltpu.make_async_remote_copy(
            ref, ref, z_send.at[target], z_recv.at[zz], device_id={"sp": target * ny + yy}
        )

    def z_arrival(source):
        ref = zbuf.at[source]
        return pltpu.make_async_remote_copy(
            ref, ref, z_send.at[source], z_recv.at[source], device_id={"sp": source * ny + yy}
        )

    rim_copy = pltpu.make_async_remote_copy(
        tail, rim, rim_send.at[0], rim_recv.at[0], device_id={"sp": place + 1}
    )
    rim_arrival = pltpu.make_async_remote_copy(
        tail, rim, rim_send.at[0], rim_recv.at[0], device_id={"sp": place - 1}
    )

    def block_copy(kind, t, origin, target, recv):
        lanes = pl.ds(pl.multiple_of((kind * tp + origin) * GROUP, GROUP), GROUP)
        ref = mixed.at[t, :, lanes]
        return pltpu.make_async_remote_copy(
            ref, ref, blk_send.at[0], recv.at[kind, t], device_id={"tp": target}
        )

    def relay_first(kind, t):
        landed(mixed.at[t, :, 0 : 2 * GROUP], blk_send.at[0], near_recv.at[kind, t]).wait_recv()
        block_copy(kind, t, behind, ahead, far_recv).start()
        block_copy(kind, t, behind, partner, pair_recv).start()
        block_copy(kind, t, ahead, partner, pair_recv).start()

    def relay_second(kind, t):
        landed(mixed.at[t, :, 0:GROUP], blk_send.at[0], far_recv.at[kind, t]).wait_recv()
        block_copy(kind, t, far, partner, pair_recv).start()

    def pair_wait(kind, t):
        half = mixed.at[t, :, 0 : tp // 2 * GROUP]
        landed(half, blk_send.at[0], pair_recv.at[kind, t]).wait_recv()

    blocks_sent = landed(
        mixed.at[:, :, 0 : 2 * (tp - 1) * GROUP], blk_send.at[0], pair_recv.at[0, 0]
    )

    def put(kind, t, value):
        lanes = pl.ds(pl.multiple_of((kind * tp + me) * GROUP, GROUP), GROUP)
        mixed[t, :, lanes] = value

    smalls[0].start()
    tok_copy(0).start()
    w_copy(0).start()
    w_copy(1).start()
    smalls[1].start()
    barrier = pltpu.get_barrier_semaphore()
    for k in range(1, tp):
        pl.semaphore_signal(barrier, inc=1, device_id={"tp": lax.rem(me + k, tp)})
    for r in range(1, ny):
        pl.semaphore_signal(barrier, inc=1, device_id={"sp": zz * ny + lax.rem(yy + r, ny)})

    def greet_z(target, _):
        pl.semaphore_signal(barrier, inc=1, device_id={"sp": target * ny + yy})
        return 0

    lax.fori_loop(zz + 1, nz, greet_z, 0)

    @pl.when(jnp.logical_and(yy == ny - 1, zz < nz - 1))
    def _():
        pl.semaphore_signal(barrier, inc=1, device_id={"sp": place + 1})

    for t in range(1, nb):
        tok_copy(t).start()
    smalls[2].start()

    def meet():
        with scope("barrier"):
            across = jnp.where(yy == 0, jnp.minimum(zz, 1), 0)
            pl.semaphore_wait(barrier, tp + ny - 2 + zz + across)

        def ready(target, _):
            pl.semaphore_signal(ready_z.at[0], inc=1, device_id={"sp": target * ny + yy})
            return 0

        lax.fori_loop(0, zz, ready, 0)

        @pl.when(jnp.logical_and(yy == 0, zz > 0))
        def _():
            pl.semaphore_signal(ready_rim.at[0], inc=1, device_id={"sp": place - 1})

        for kind in range(2):
            for k in range(tp - 2):
                far_cols(kind, k).start()
        for kind in range(2):
            partner_cols(kind).start()
            own_cols(kind).start()

    row = lax.broadcasted_iota(jnp.int32, (CHUNK, CHUNK), 0)
    col = lax.broadcasted_iota(jnp.int32, (CHUNK, CHUNK), 1)
    causal = row >= col
    ones = causal.astype(bf16)

    def lanes(first, last):
        return slice(first * GROUP, last * GROUP)

    def span(t):
        return slice(t * ROWS, (t + 1) * ROWS)

    def prepare(t):
        gain = gainv[...].astype(bf16)
        for r in range(t * ROWS, (t + 1) * ROWS, STRIP):
            raw = tok[r : r + STRIP, :]
            feats = raw.shape[1]
            tok[r : r + STRIP, :] = raw * gain
            squares = raw * raw
            squares = squares[:, : feats // 2] + squares[:, feats // 2 :]
            squares = squares[:, : feats // 4] + squares[:, feats // 4 :]
            mean = jnp.sum(squares.astype(f32), axis=1, keepdims=True) * (1.0 / feats)
            scl[r : r + STRIP, :] = jnp.broadcast_to(lax.rsqrt(mean + norm_eps), (STRIP, GROUP))

    def project_states(t):
        here = span(t)
        both = dot(tok[here, :], w[:, lanes(0, 2)])
        scale = scl[here, :]
        xs[here, :] = (both[:, :GROUP] * scale).astype(bf16)
        val[here, :] = (both[:, GROUP:] * scale).astype(bf16)

    def logs(t):
        here = span(t)
        key = (1.0 - floorv[...]) * jax.nn.sigmoid(-xs[here, :].astype(f32))
        keyv[here, :] = key
        hi, low = split(jnp.log(1.0 - key) + leakv[here, :])
        terms[here, :GROUP] = hi
        terms[here, GROUP:] = low

    def piece(chunk):
        return slice(chunk * CHUNK, (chunk + 1) * CHUNK)

    def sums(chunk):
        both = dot(ones, terms[piece(chunk), :])
        emid[piece(chunk), :] = both[:, :GROUP] + both[:, GROUP:]

    def decays(chunk):
        at = piece(chunk)
        cum = emid[at, :]
        mid = cum[CHUNK // 2 - 1 : CHUNK // 2]
        last = cum[CHUNK - 1 : CHUNK]
        stats[chunk, 0:1] = mid
        stats[chunk, 2:3] = last
        emid[at, :] = jnp.exp(cum - mid)
        k_mid = keyv[at, :] * jnp.exp(mid - cum)
        kmid[at, :] = k_mid.astype(bf16)
        kend[at, :] = (k_mid * jnp.exp(last - mid)).astype(bf16)

    def own_state():
        state, offset = jnp.zeros((GROUP, GROUP), f32), jnp.zeros((1, GROUP), f32)
        for chunk in range(nchunk):
            at, last = piece(chunk), stats[chunk, 2:3]
            old[chunk] = state.astype(bf16)
            stats[chunk, 1:2] = offset
            state = state * jnp.exp(last) + dot(val[at, :], kend[at, :], ((0,), (0,)))
            offset = offset + last
        return state, offset

    def gated_inputs(both, factor):
        left = (both[:, :GROUP] * factor).astype(bf16).astype(f32)
        right = (both[:, GROUP:] * factor).astype(bf16).astype(f32)
        return (left * right).astype(bf16).astype(f32)

    with scope("load0"):
        smalls[0].wait()
        tok_copy(0).wait()
    for i in range(2, 7):
        w_copy(i).start()
    for copy in smalls[3:]:
        copy.start()
    with scope("prep0"):
        prepare(0)
    with scope("load1"):
        w_wait(0, 2)
        smalls[1].wait()
    for t in range(1, nb):
        with scope("tokwait"):
            tok_copy(t).wait()
        with scope("A"):
            project_states(t - 1)
            prepare(t)
        if t == 2:
            meet()

    def pack(slot, matrix, logs):
        hi = logs.astype(bf16)
        mid, low = split(logs - hi.astype(f32))
        slot[0:GROUP, :] = matrix.astype(bf16)
        r = lax.broadcasted_iota(jnp.int32, (LOGS, GROUP), 0)
        rows = jnp.where(r == 0, hi.astype(f32), jnp.where(r == 1, mid.astype(f32), low.astype(f32)))
        slot[GROUP : GROUP + LOGS, :] = rows.astype(bf16)

    def unpack(slot):
        logs = slot[GROUP : GROUP + LOGS, :].astype(f32)
        return slot[0:GROUP, :].astype(f32), logs[0:1] + logs[1:2] + logs[2:3]

    pad[0:HALO, :] = jnp.zeros((HALO, GROUP), f32)

    def convolve(first, size, conv_in, proj_b):
        taps_f = tapsv[...].astype(f32)
        total = taps_f[TAPS - 1 : TAPS] * conv_in
        for j in range(TAPS - 1):
            start = HALO - (TAPS - 1) + j + first
            total += taps_f[j : j + 1] * pad[start : start + size, :]
        return (rms(proj_b * total) * ggainv[...]).astype(bf16)

    def project_inputs(t):
        here = span(t)
        pad[HALO + t * ROWS : HALO + (t + 1) * ROWS, :] = gated_inputs(
            dot(tok[here, :], w[:, lanes(2, 4)]), scl[here, :]
        )

    def project_gates(t):
        here = span(t)
        both = dot(tok[here, :], w[:, lanes(4, 6)])
        factor = scl[here, :]
        prods[here, :] = (both[:, :GROUP] * factor).astype(bf16)
        gate[here, :] = (both[:, GROUP:] * factor).astype(bf16)

    def project_query(t):
        here = span(t)
        wide[here, :] = (dot(tok[here, :], w[:, lanes(6, 7)]) * scl[here, :]).astype(bf16)

    def send(kind, t):
        block_copy(kind, t, me, ahead, near_recv).start()
        block_copy(kind, t, me, behind, near_recv).start()
        block_copy(kind, t, me, partner, pair_recv).start()

    def conv(t):
        conv_in = pad[HALO + t * ROWS : HALO + (t + 1) * ROWS, :]
        put(1, t, convolve(t * ROWS, ROWS, conv_in, prods[span(t), :].astype(f32)))

    def reads(chunk):
        at = slice(chunk * CHUNK, (chunk + 1) * CHUNK)
        query = jax.nn.silu(wide[at, :].astype(f32))
        mid, before = stats[chunk, 0:1], stats[chunk, 1:2]
        q_mid = query * emid[at, :]
        q_all = q_mid * jnp.exp(mid)
        qdev[at, :] = (q_all * jnp.exp(before)).astype(bf16)
        scores = dot(q_mid.astype(bf16), kmid[at, :], ((1,), (1,)))
        scores = jnp.where(causal, scores, 0.0).astype(bf16)
        read[at, :] = dot(scores, val[at, :]) + dot(q_all.astype(bf16), old[chunk], ((1,), (1,)))

    def combine():
        with scope("ywait"):
            y_all.wait_recv()
        whole, logs = unpack(ybuf.at[0])
        for j in range(1, ny):
            more, log = unpack(ybuf.at[j])
            whole = whole * jnp.exp(log) + more
            logs = logs + log
        pack(zbuf.at[zz], whole, logs)
        with scope("readyz"):
            @pl.when(zz < nz - 1)
            def _():
                pl.semaphore_wait(ready_z.at[0], nz - 1 - zz)

        def send_z(step, _):
            z_copy(nz - 1 - step).start()
            return 0

        lax.fori_loop(0, nz - 1 - zz, send_z, 0)

    def first_rows():
        with scope("rimwait"):
            @pl.when(place > 0)
            def _():
                rim_arrival.wait_recv()
                pad[0:HALO, :] = rim[...]

        conv(0)
        send(1, 0)

    def share():
        with scope("colxwait"):
            far_cols_in.wait_recv()
        share_all(yy, y_ahead, 0)
        share_all(yy, y_behind, 1)

    def share_on():
        with scope("colywait"):
            shared_in(0).wait_recv()
        share_all(y_behind, y_ahead, 2)

    with scope("w23wait"):
        w_wait(2, 4)
        smalls[2].wait()
    with scope("A2"):
        project_states(nb - 1)
        logs(0)
        logs(1)
        project_inputs(nb - 1)
        logs(2)
        logs(3)
        tail[...] = pad[count : count + HALO, :]
        project_inputs(0)
        for chunk in range(nchunk):
            sums(chunk)
        for chunk in range(nchunk):
            decays(chunk)
        project_inputs(1)
        pack(ybuf.at[yy], *own_state())
    with scope("rimsend"):
        @pl.when(jnp.logical_and(yy == ny - 1, zz < nz - 1))
        def _():
            pl.semaphore_wait(ready_rim.at[0], 1)

        @pl.when(place < sp - 1)
        def _():
            rim_copy.start()

        for r in range(1, ny):
            y_copy(r).start()

    with scope("w46wait"):
        w_wait(4, 6)
        w_wait(6, 7)
        for copy in smalls[3:]:
            copy.wait()
    with scope("B1"):
        project_gates(1)
        conv(1)
        project_gates(0)
        send(1, 1)
    with scope("B2"):
        project_inputs(2)
        project_gates(2)
        conv(2)
        project_query(0)
        send(1, 2)
    first_rows()
    with scope("B3"):
        project_gates(3)
        conv(3)
        reads(0)
        reads(1)
        send(1, 3)
    combine()
    share()
    with scope("C2"):
        project_query(1)
        project_query(2)
        reads(2)
        reads(3)
        project_query(3)
        reads(4)
        reads(5)
    with scope("C3"):
        reads(6)
        reads(7)

    conv_order = [1, 2, 0, 3]
    with scope("relayconv"):
        for t in conv_order:
            relay_first(1, t)

    incoming[...] = jnp.zeros_like(incoming)

    def hop_z(source, _):
        z_arrival(source).wait_recv()
        matrix, log = unpack(zbuf.at[source])
        incoming[...] = incoming[...] * jnp.exp(log) + matrix
        return 0

    with scope("hopz"):
        lax.fori_loop(0, zz, hop_z, 0)

    def hop_y(source, _):
        matrix, log = unpack(ybuf.at[source])
        incoming[...] = incoming[...] * jnp.exp(log) + matrix
        return 0

    lax.fori_loop(0, yy, hop_y, 0)

    def merge(t):
        here = span(t)
        total = read[here, :] + dot(qdev[here, :], incoming[...].astype(bf16), ((1,), (1,)))
        out = rms(total) * sgainv[...] * jax.nn.silu(gate[here, :].astype(f32))
        put(0, t, out.astype(bf16))

    with scope("merge"):
        merge(0)
        send(0, 0)
        for t in range(1, nb):
            merge(t)
        for t in range(1, nb):
            send(0, t)

    def conv_dot(t):
        with scope("convdot"):
            pair_wait(1, t)
            side = cols[tp : 2 * tp].reshape(tp * GROUP, ncols)
            acc[span(t), :] = dot(mixed[t, :, tp * GROUP :], side)

    share_on()
    with scope("relayconv2"):
        for t in conv_order[:-1]:
            relay_second(1, t)
    with scope("relaystate"):
        relay_first(0, 0)
    with scope("relayconv2last"):
        relay_second(1, conv_order[-1])
    with scope("colwait"):
        own_cols_done.wait()
        partner_cols_in.wait_recv()
        shared_in(1).wait_recv()
        shared_in(2).wait_recv()
    conv_dot(conv_order[0])
    conv_dot(conv_order[1])
    with scope("relaystate"):
        relay_first(0, 1)
    conv_dot(conv_order[2])
    for t in range(2, nb):
        with scope("relaystate"):
            relay_first(0, t)
    conv_dot(conv_order[3])

    def finish(t):
        with scope("finwait"):
            pair_wait(0, t)
        with scope("findot"):
            main = cols[0:tp].reshape(tp * GROUP, ncols)
            total = acc[span(t), :] + dot(mixed[t, :, : tp * GROUP], main)
            result[span(t), :] = total.astype(bf16)

    for t in range(nb):
        with scope("finfar"):
            relay_second(0, t)
        if t > 0:
            finish(t - 1)
    finish(nb - 1)

    with scope("drain"):
        blocks_sent.wait_send()
        colx_sent.wait_send()
        shares_sent.wait_send()
        y_all.wait_send()

        def drain_z(target, _):
            z_copy(target).wait_send()
            return 0

        lax.fori_loop(zz + 1, nz, drain_z, 0)

        @pl.when(place < sp - 1)
        def _():
            rim_copy.wait_send()


def body(
    tokens, in_gain, w_query, w_forget, w_input, w_outgate, w_conv_h, w_conv_b, w_conv_c,
    forget_floor, forget_leak, state_gain, conv_taps, group_gain, out_state, out_conv,
):
    count, feats = tokens.shape
    tp, sp = lax.axis_size("tp"), lax.axis_size("sp")
    ny, nz = NY, sp // NY
    ncols, nb = out_state.shape[1] // tp, count // ROWS
    nchunk = count // CHUNK
    hbm, vmem = pl.BlockSpec(memory_space=pltpu.HBM), pl.BlockSpec(memory_space=pltpu.VMEM)
    sems = pltpu.SemaphoreType.DMA
    return pl.pallas_call(
        functools.partial(fused_kernel, tp, ny, nz),
        in_specs=[hbm] * 16,
        out_specs=vmem,
        out_shape=jax.ShapeDtypeStruct((count, ncols), bf16),
        scratch_shapes=[
            pltpu.VMEM((count, feats), bf16),
            pltpu.VMEM((feats, 7 * GROUP), bf16),
            pltpu.VMEM((count, GROUP), f32),
            pltpu.VMEM((2 * tp, GROUP, ncols), bf16),
            pltpu.VMEM((nb, ROWS, 2 * tp * GROUP), bf16),
            pltpu.VMEM((count, GROUP), bf16),
            pltpu.VMEM((count, GROUP), bf16),
            pltpu.VMEM((count, GROUP), bf16),
            pltpu.VMEM((count, GROUP), f32),
            pltpu.VMEM((nchunk, GROUP, GROUP), bf16),
            pltpu.VMEM((nchunk, HALO, GROUP), f32),
            pltpu.VMEM((count, GROUP), bf16),
            pltpu.VMEM((count, GROUP), f32),
            pltpu.VMEM((count, GROUP), bf16),
            pltpu.VMEM((count, GROUP), f32),
            pltpu.VMEM((count, ncols), f32),
            pltpu.VMEM((1, feats), f32),
            pltpu.VMEM((1, GROUP), f32),
            pltpu.VMEM((1, GROUP), f32),
            pltpu.VMEM((1, GROUP), f32),
            pltpu.VMEM((TAPS, GROUP), bf16),
            pltpu.VMEM((count, GROUP), bf16),
            pltpu.VMEM((count, GROUP), bf16),
            pltpu.VMEM((count, GROUP), f32),
            pltpu.VMEM((count, 2 * GROUP), bf16),
            pltpu.VMEM((count, GROUP), bf16),
            pltpu.VMEM((HALO + count, GROUP), f32),
            pltpu.VMEM((GROUP, GROUP), f32),
            pltpu.VMEM((ny, GROUP + LOGS, GROUP), bf16),
            pltpu.VMEM((nz, GROUP + LOGS, GROUP), bf16),
            pltpu.VMEM((HALO, GROUP), f32),
            pltpu.VMEM((HALO, GROUP), f32),
            sems((nb,)), sems((4,)), sems((6,)), sems((1,)),
            pltpu.SemaphoreType.REGULAR((1,)), pltpu.SemaphoreType.REGULAR((1,)),
            sems((1,)), sems((2,)), sems((1,)), sems((3,)),
            sems((1,)), sems((1,)), sems((nz,)), sems((nz,)), sems((1,)), sems((1,)),
            sems((1,)), sems((2, nb)), sems((2, nb)), sems((2, nb)),
        ],
        compiler_params=pltpu.CompilerParams(
            vmem_limit_bytes=40 * 2**20, collective_id=0, has_side_effects=True
        ),
    )(*[pltpu.with_memory_space_constraint(a, pltpu.HBM) for a in (
        tokens, in_gain[None], w_query, w_forget, w_input, w_outgate, w_conv_h, w_conv_b, w_conv_c,
        forget_floor[None], forget_leak, state_gain[None], conv_taps, group_gain[None],
        out_state, out_conv,
    )])


def solution(mesh):
    cols, rows = P(None, "tp"), P("tp", None)
    in_specs = (
        P("sp", None), P(), cols, cols, cols, cols, cols, cols, cols,
        P("tp"), P("sp", "tp"), P(), cols, P(), rows, rows,
    )
    return jax.shard_map(
        body, mesh=mesh, in_specs=in_specs, out_specs=P("sp", "tp"), check_vma=False
    )
```
